512 devices in a mesh: fs: 64 (over z, y), tp: 8 (over x, core).
Axes of the slice: x: 4, y: 8, z: 8, core: 2. Of those that a mesh axis runs over, the one named last changes fastest.
Arguments:
- x_late: bfloat16 [16384, 2048], P('fs'), may hold values from -6 to 6
- x_early: bfloat16 [16384, 2048], P('fs'), may hold values from -6 to 6
- cotangent: bfloat16 [16384, 2048], P('fs'), may hold values from -16 to 16
- w_gate: bfloat16 [2048, 4096], P('fs', 'tp'), may hold values from -0.125 to 0.125
- w_up: bfloat16 [2048, 4096], P('fs', 'tp'), may hold values from -0.125 to 0.125
- w_down: bfloat16 [4096, 2048], P('tp', 'fs'), may hold values from -0.09375 to 0.09375
- conv_taps: float32 [3, 4096], replicated, may hold values from -3 to 3
- conv_bias: float32 [4096], replicated, may hold values from -3 to 3
- grad_down: float32 [4096, 2048], P('tp', 'fs'), may hold values from -60 to 60
Outputs:
- y_late: bfloat16 [16384, 2048], P('fs')
- dx_early: bfloat16 [16384, 2048], P('fs')
- grad_down_out: float32 [4096, 2048], P('tp', 'fs')
The draws below stay inside these ranges and needn't reach their ends.
All inputs are finite; a program needn't handle non-finite values.
Results may differ from the reference program's by a relative error of at most 0.017.
Values may be sent and summed in bfloat16 or wider, within the bound.
No kernel may reach another device: no remote copies, remote signals or barrier semaphores. Data moves between devices by JAX's collectives and lax.ppermute only.
A program may use at most 128 MiB of HBM per device.

```python
import jax
import jax.numpy as jnp
from jax import lax

D = 2048
FF = 4096
TAPS = 3
TOK_DEV = 256
TOKENS = 16384
N_FS = 64
N_TP = 8


def strengthened(array, stream_key, source, target, blocks, factor):
    owner, partner = [(jnp.arange(array.shape[dim]) // (array.shape[dim] // blocks)).reshape([-1 if axis == dim else 1 for axis in range(array.ndim)]) for dim in (source, target)]
    chosen = jax.random.permutation(stream_key, blocks)[partner]
    strong = (owner == chosen) | (owner == (partner + blocks // 2) % blocks)
    return jnp.where(strong, factor * array, array)


def shard_levels(rng, dims, shards, smallest, top_value):
    level, own = 1.0, jax.random.fold_in(rng, 6)
    for axis_at, parts in shards:
        steps = jnp.exp(jax.random.uniform(jax.random.fold_in(own, axis_at), (parts,), jnp.float32, smallest / len(shards), top_value / len(shards)))
        level = level * jnp.repeat(steps, dims[axis_at] // parts).reshape([-1 if axis == axis_at else 1 for axis in range(len(dims))])
    return level


def scatter_about(rng, dims, spread, bound, cuts=(), dtype=jnp.bfloat16):
    loudness = shard_levels(rng, dims, cuts, -0.22, 0.18) if cuts else 1.0
    array = jax.random.normal(rng, dims, jnp.float32) * spread * loudness
    return jnp.minimum(jnp.maximum(array, -bound), bound).astype(dtype)


def bell_draw_with(key, dims, scale, bound, split, heavy, held_as=jnp.bfloat16):
    values = scale * jax.random.normal(key, dims, jnp.float32)
    if split:
        values = values * shard_levels(key, dims, split, -0.22, 0.18)
    return jnp.clip(strengthened(values, jax.random.fold_in(key, 3), *heavy), -bound, bound).astype(held_as)


def setup_inputs(seed: int = 0) -> dict:
    streams_of = jax.random.split(jax.random.key(seed), 10)
    x_late = scatter_about(streams_of[0], (TOKENS, D), 1.0, 6.0, ((0, 64),))
    x_early = scatter_about(streams_of[1], (TOKENS, D), 1.0, 6.0, ((0, 64),))
    cotangent = bell_draw_with(streams_of[2], (TOKENS, D), 1.0, 16.0, ((0, 64),), (0, 1, 64, 4.0))
    w_gate = scatter_about(streams_of[3], (D, FF), D ** -0.5, 0.125, ((0, 64), (1, 8)))
    w_up = scatter_about(streams_of[4], (D, FF), D ** -0.5, 0.125, ((0, 64), (1, 8)))
    w_down = scatter_about(streams_of[5], (FF, D), FF ** -0.5, 0.09375, ((0, 8), (1, 64)))
    conv_taps = scatter_about(streams_of[6], (TAPS, FF), 0.6, 3.0, (), jnp.float32)
    conv_bias = scatter_about(streams_of[7], (FF,), 0.5, 3.0, (), jnp.float32)
    grad_down = scatter_about(streams_of[8], (FF, D), 10.0, 60.0, ((0, 8), (1, 64)), jnp.float32)
    return {"x_late": x_late, "x_early": x_early, "cotangent": cotangent, "w_gate": w_gate, "w_up": w_up, "w_down": w_down, "conv_taps": conv_taps, "conv_bias": conv_bias, "grad_down": grad_down}


def shift_later(field, steps):
    pad = jnp.zeros((field.shape[0], steps, field.shape[2]), jnp.float32)
    return jnp.concatenate([pad, field[:, :field.shape[1] - steps]], axis=1)


def shift_earlier(field, steps):
    pad = jnp.zeros((field.shape[0], steps, field.shape[2]), jnp.float32)
    return jnp.concatenate([field[:, steps:], pad], axis=1)


def mlp_parts(inputs, w_gate, w_up, conv_taps, conv_bias):
    gate = jnp.dot(inputs, w_gate, preferred_element_type=jnp.float32).astype(jnp.bfloat16)
    up = jnp.dot(inputs, w_up, preferred_element_type=jnp.float32)
    seqs = gate.astype(jnp.float32).reshape(N_FS, TOK_DEV, FF)
    conv = conv_bias + conv_taps[2] * seqs + conv_taps[1] * shift_later(seqs, 1) + conv_taps[0] * shift_later(seqs, 2)
    conv = conv.reshape(TOKENS, FF)
    act = jax.nn.silu(conv)
    hidden = (act * up).astype(jnp.bfloat16)
    return conv, act, up, hidden


def rounded(value):
    return lax.optimization_barrier(value.astype(jnp.bfloat16)).astype(jnp.float32)


def reference(x_late, x_early, cotangent, w_gate, w_up, w_down, conv_taps, conv_bias, grad_down):
    width = FF // N_TP
    conv, act, up, hidden = mlp_parts(x_late, w_gate, w_up, conv_taps, conv_bias)
    total = jnp.zeros((TOKENS, D), jnp.float32)
    for block in range(N_TP):
        lo = block * width
        total = total + rounded(jnp.dot(hidden[:, lo:lo + width], w_down[lo:lo + width], preferred_element_type=jnp.float32))
    y_late = total.astype(jnp.bfloat16)

    conv, act, up, hidden = mlp_parts(x_early, w_gate, w_up, conv_taps, conv_bias)
    dhidden = jnp.dot(cotangent, w_down.T, preferred_element_type=jnp.float32)
    dup = (dhidden * act).astype(jnp.bfloat16)
    sig = jax.nn.sigmoid(conv)
    dconv = (dhidden * up * sig * (1.0 + conv * (1.0 - sig))).reshape(N_FS, TOK_DEV, FF)
    dgate = conv_taps[2] * dconv + conv_taps[1] * shift_earlier(dconv, 1) + conv_taps[0] * shift_earlier(dconv, 2)
    dgate = dgate.reshape(TOKENS, FF).astype(jnp.bfloat16)
    total = jnp.zeros((TOKENS, D), jnp.float32)
    for block in range(N_TP):
        lo = block * width
        part = jnp.dot(dup[:, lo:lo + width], w_up[:, lo:lo + width].T, preferred_element_type=jnp.float32)
        part = part + jnp.dot(dgate[:, lo:lo + width], w_gate[:, lo:lo + width].T, preferred_element_type=jnp.float32)
        total = total + rounded(part)
    dx_early = total.astype(jnp.bfloat16)
    grad_down_out = grad_down + jnp.dot(hidden.T, cotangent, preferred_element_type=jnp.float32)
    return y_late, dx_early, grad_down_out
```

```python
import jax
import jax.numpy as jnp
from jax import lax
from jax.experimental import pallas as pl
from jax.experimental.pallas import tpu as pltpu
from jax.sharding import Mesh
from jax.sharding import PartitionSpec as P

AXES = ("z", "y", "x", "c")
FS = ("z", "y")
TP = ("x", "c")
NZ, NY, NX, NC = 8, 8, 4, 2
UNITS = 512
TOK = 256
WIDTH = 2048


def place(z, y, x, c):
    return ((z * NY + y) * NX + x) * NC + c


def split_groups(core_along_y):
    groups = []
    for x in range(NX):
        for k in range(8):
            groups.append([place(k, y, x, core_along_y) for y in range(NY)])
            groups.append([place(z, k, x, 1 - core_along_y) for z in range(NZ)])
    return groups


FIRST = split_groups(0)
SECOND = split_groups(1)


def contract_last(left, right):
    return lax.dot_general(
        left, right, (((1,), (1,)), ((), ())), preferred_element_type=jnp.float32
    )


def shift_later(field, steps):
    row = lax.broadcasted_iota(jnp.int32, field.shape, 0)
    return jnp.where(row >= steps, pltpu.roll(field, steps, 0), 0.0)


def shift_earlier(field, steps):
    rows = field.shape[0]
    row = lax.broadcasted_iota(jnp.int32, field.shape, 0)
    return jnp.where(row < rows - steps, pltpu.roll(field, rows - steps, 0), 0.0)


def layer_kernel(
    stride_ref, xl_ref, xe_ref, cot_ref, cot_t_ref, taps_ref, bias_ref, w_hbm,
    y_ref, dx_ref, grad_ref, w_ref, sems,
):
    outer = stride_ref[0]
    inner = stride_ref[1]

    def copy(p, j):
        at = pl.multiple_of((p * outer + j * inner) * 32, 32)
        return pltpu.make_async_copy(w_hbm.at[p, j], w_ref.at[pl.ds(at, 32)], sems.at[p, j])

    for p in range(8):
        for j in range(8):
            copy(p, j).start()
    t0, t1, t2 = taps_ref[0:1, :], taps_ref[1:2, :], taps_ref[2:3, :]
    bias = bias_ref[0:1, :]
    for p in range(8):
        for j in range(8):
            copy(p, j).wait()
    w_gate = w_ref[:, 0:UNITS]
    w_up = w_ref[:, UNITS : 2 * UNITS]
    w_down = w_ref[:, 2 * UNITS : 3 * UNITS]

    def hidden_parts(x):
        gate = jnp.dot(x, w_gate, preferred_element_type=jnp.float32)
        gate = gate.astype(jnp.bfloat16).astype(jnp.float32)
        up = jnp.dot(x, w_up, preferred_element_type=jnp.float32)
        conv = bias + t2 * gate + t1 * shift_later(gate, 1) + t0 * shift_later(gate, 2)
        sig = 1.0 / (1.0 + jnp.exp(-conv))
        act = conv * sig
        return conv, sig, act, up, (act * up).astype(jnp.bfloat16)

    conv, sig, act, up, hidden = hidden_parts(xe_ref[...])
    for k in range(8):
        part = jnp.dot(
            cot_t_ref[k * 256 : (k + 1) * 256, :], hidden, preferred_element_type=jnp.float32
        ).astype(jnp.bfloat16)
        for j in range(8):
            at = pl.multiple_of((k * outer + j * inner) * 32, 32)
            grad_ref[pl.ds(at, 32), :] = part[j * 32 : (j + 1) * 32, :]
    dhidden = jnp.dot(cot_ref[...], w_down, preferred_element_type=jnp.float32)
    dup = (dhidden * act).astype(jnp.bfloat16)
    dconv = dhidden * up * sig * (1.0 + conv * (1.0 - sig))
    dgate = t2 * dconv + t1 * shift_earlier(dconv, 1) + t0 * shift_earlier(dconv, 2)
    dgate = dgate.astype(jnp.bfloat16)
    dx_ref[...] = (contract_last(dup, w_up) + contract_last(dgate, w_gate)).astype(jnp.bfloat16)
    late = hidden_parts(xl_ref[...])[4]
    y_ref[...] = contract_last(late, w_down).astype(jnp.bfloat16)


def layer(strides, x_late, x_early, cot, cot_t, taps, bias, w):
    vmem = pl.BlockSpec(memory_space=pltpu.VMEM)
    return pl.pallas_call(
        layer_kernel,
        out_shape=(
            jax.ShapeDtypeStruct((TOK, WIDTH), jnp.bfloat16),
            jax.ShapeDtypeStruct((TOK, WIDTH), jnp.bfloat16),
            jax.ShapeDtypeStruct((WIDTH, UNITS), jnp.bfloat16),
        ),
        in_specs=[pl.BlockSpec(memory_space=pltpu.SMEM)] + [vmem] * 6
        + [pl.BlockSpec(memory_space=pl.ANY)],
        out_specs=(vmem, vmem, vmem),
        scratch_shapes=[
            pltpu.VMEM((WIDTH, 3 * UNITS), jnp.bfloat16),
            pltpu.SemaphoreType.DMA((8, 8)),
        ],
        compiler_params=pltpu.CompilerParams(vmem_limit_bytes=48 * 1024 * 1024),
        name="layer",
    )(strides, x_late, x_early, cot, cot_t, taps, bias, w)


def exchanged(value):
    return lax.ppermute(value, "c", [(0, 1), (1, 0)])


def f32_sum(pieces):
    return pieces.astype(jnp.float32).sum(axis=0).astype(jnp.bfloat16)


def shards(x_late, x_early, cotangent, w_gate, w_up, w_down, conv_taps, conv_bias, grad_down):
    core = lax.axis_index("c")
    offset = lax.axis_index(TP) * UNITS
    taps = lax.dynamic_slice_in_dim(conv_taps, offset, UNITS, 1)
    bias = lax.dynamic_slice_in_dim(conv_bias, offset, UNITS, 0)[None]
    mine = jnp.concatenate([w_gate, w_up, w_down.T], axis=1)
    near = lax.all_to_all(
        jnp.broadcast_to(mine[None], (8,) + mine.shape), AXES, 0, 0,
        tiled=True, axis_index_groups=FIRST,
    )
    w = lax.all_gather(near, AXES, axis_index_groups=SECOND)
    strides = jnp.where(core == 0, jnp.array([8, 1]), jnp.array([1, 8])).astype(jnp.int32)
    y_part, dx_part, grad_part = layer(
        strides, x_late, x_early, cotangent, cotangent.T, taps, bias, w
    )

    grad = lax.all_to_all(
        grad_part.reshape(8, 256, UNITS), AXES, 0, 0, tiled=True, axis_index_groups=SECOND
    )
    grad = f32_sum(grad).reshape(8, 32, UNITS)
    grad = lax.all_to_all(grad, AXES, 0, 0, tiled=True, axis_index_groups=FIRST)
    grad_down_out = grad_down + grad.astype(jnp.float32).sum(axis=0).T

    halves = jnp.stack([y_part.reshape(2, 128, WIDTH), dx_part.reshape(2, 128, WIDTH)], axis=1)
    keep = lax.dynamic_index_in_dim(halves, core, 0, keepdims=False)
    give = lax.dynamic_index_in_dim(halves, 1 - core, 0, keepdims=False)
    chip = (keep.astype(jnp.float32) + exchanged(give).astype(jnp.float32)).astype(jnp.bfloat16)
    pieces = chip.reshape(2, NX, 32, WIDTH).swapaxes(0, 1)
    total = f32_sum(lax.all_to_all(pieces, "x", 0, 0, tiled=True))
    total = lax.all_to_all(
        jnp.broadcast_to(total[None], (NX, 2, 32, WIDTH)), "x", 0, 0, tiled=True
    )
    total = total.swapaxes(0, 1).reshape(2, 128, WIDTH)
    other = exchanged(total)
    first = jnp.where(core == 0, total, other)
    second = jnp.where(core == 0, other, total)
    y_late = jnp.concatenate([first[0], second[0]], axis=0)
    dx_early = jnp.concatenate([first[1], second[1]], axis=0)
    return (y_late, dx_early, grad_down_out)


def solution(mesh):
    torus = Mesh(mesh.devices.reshape(NZ, NY, NX, NC), AXES)
    return jax.shard_map(
        shards,
        mesh=torus,
        in_specs=(
            P(FS, None),
            P(FS, None),
            P(FS, None),
            P(FS, TP),
            P(FS, TP),
            P(TP, FS),
            P(),
            P(),
            P(TP, FS),
        ),
        out_specs=(P(FS, None), P(FS, None), P(TP, FS)),
        check_vma=False,
    )
```

```python
import jax
import jax.numpy as jnp
from jax import lax
from jax.experimental import pallas as pl
from jax.experimental.pallas import tpu as pltpu
from jax.sharding import Mesh
from jax.sharding import PartitionSpec as P

AXES = ("z", "y", "x", "c")
FS = ("z", "y")
TP = ("x", "c")
NZ, NY, NX, NC = 8, 8, 4, 2
UNITS = 512
TOK = 256
WIDTH = 2048


def place(z, y, x, c):
    return ((z * NY + y) * NX + x) * NC + c


def split_groups(core_along_y):
    groups = []
    for x in range(NX):
        for k in range(8):
            groups.append([place(k, y, x, core_along_y) for y in range(NY)])
            groups.append([place(z, k, x, 1 - core_along_y) for z in range(NZ)])
    return groups


FIRST = split_groups(0)
SECOND = split_groups(1)


def contract_last(left, right):
    return lax.dot_general(
        left, right, (((1,), (1,)), ((), ())), preferred_element_type=jnp.float32
    )


def shift_later(field, steps):
    row = lax.broadcasted_iota(jnp.int32, field.shape, 0)
    return jnp.where(row >= steps, pltpu.roll(field, steps, 0), 0.0)


def shift_earlier(field, steps):
    rows = field.shape[0]
    row = lax.broadcasted_iota(jnp.int32, field.shape, 0)
    return jnp.where(row < rows - steps, pltpu.roll(field, rows - steps, 0), 0.0)


def hidden_parts(x, w_ref, taps_ref, bias_ref):
    t0, t1, t2 = taps_ref[0:1, :], taps_ref[1:2, :], taps_ref[2:3, :]
    gate = jnp.dot(x, w_ref[:, 0:UNITS], preferred_element_type=jnp.float32)
    gate = gate.astype(jnp.bfloat16).astype(jnp.float32)
    up = jnp.dot(x, w_ref[:, UNITS : 2 * UNITS], preferred_element_type=jnp.float32)
    conv = bias_ref[0:1, :] + t2 * gate + t1 * shift_later(gate, 1) + t0 * shift_later(gate, 2)
    return conv, up


def sigmoid(v):
    return 1.0 / (1.0 + jnp.exp(-v))


def layer_kernel(
    stride_ref, taps_ref, bias_ref, xe_hbm, xl_hbm, cot_hbm, w_hbm,
    keep_ref, give_ref, hidden_ref,
    xe_ref, xl_ref, cot_ref, w_ref, w_sems, x_sems,
):
    outer = stride_ref[0]
    inner = stride_ref[1]
    south = outer == 8

    def w_copy(p, j, part):
        at = pl.multiple_of((p * outer + j * inner) * 32, 32)
        cols = pl.ds(0, 2 * UNITS) if part == 0 else pl.ds(2 * UNITS, UNITS)
        return pltpu.make_async_copy(
            w_hbm.at[p, j, :, cols], w_ref.at[pl.ds(at, 32), cols], w_sems.at[part, p, j]
        )

    blocks = [(p, j) for p in range(8) for j in range(8)]
    xe_copy = pltpu.make_async_copy(xe_hbm, xe_ref, x_sems.at[0])
    cot_copy = pltpu.make_async_copy(cot_hbm, cot_ref, x_sems.at[1])
    xl_copy = pltpu.make_async_copy(xl_hbm, xl_ref, x_sems.at[2])
    xe_copy.start()
    for p, j in blocks:
        w_copy(p, j, 0).start()
    cot_copy.start()
    for p, j in blocks:
        w_copy(p, j, 1).start()
    xl_copy.start()

    def put(value, at):
        value = value.astype(jnp.bfloat16)

        @pl.when(south)
        def _():
            for k in range(NX):
                keep_ref[k, at] = value[k * 32 : (k + 1) * 32]
                give_ref[k, at] = value[128 + k * 32 : 128 + (k + 1) * 32]

        @pl.when(jnp.logical_not(south))
        def _():
            for k in range(NX):
                give_ref[k, at] = value[k * 32 : (k + 1) * 32]
                keep_ref[k, at] = value[128 + k * 32 : 128 + (k + 1) * 32]

    t0, t1, t2 = taps_ref[0:1, :], taps_ref[1:2, :], taps_ref[2:3, :]
    xe_copy.wait()
    for p, j in blocks:
        w_copy(p, j, 0).wait()
    conv, up = hidden_parts(xe_ref[...], w_ref, taps_ref, bias_ref)
    sig = sigmoid(conv)
    act = conv * sig
    hidden_ref[...] = (act * up).astype(jnp.bfloat16)
    slope = up * sig * (1.0 + conv * (1.0 - sig))
    cot_copy.wait()
    for p, j in blocks:
        w_copy(p, j, 1).wait()
    w_down = w_ref[:, 2 * UNITS : 3 * UNITS]
    dhidden = jnp.dot(cot_ref[...], w_down, preferred_element_type=jnp.float32)
    dup = (dhidden * act).astype(jnp.bfloat16)
    dconv = dhidden * slope
    dgate = t2 * dconv + t1 * shift_earlier(dconv, 1) + t0 * shift_earlier(dconv, 2)
    dgate = dgate.astype(jnp.bfloat16)
    put(
        contract_last(dup, w_ref[:, UNITS : 2 * UNITS]) + contract_last(dgate, w_ref[:, 0:UNITS]),
        1,
    )
    xl_copy.wait()
    late, late_up = hidden_parts(xl_ref[...], w_ref, taps_ref, bias_ref)
    put(contract_last((late * sigmoid(late) * late_up).astype(jnp.bfloat16), w_down), 0)


VMEM = pl.BlockSpec(memory_space=pltpu.VMEM)
SMEM = pl.BlockSpec(memory_space=pltpu.SMEM)
HBM = pl.BlockSpec(memory_space=pltpu.HBM)


def layer(strides, taps, bias, x_early, x_late, cot, w):
    piece = jax.ShapeDtypeStruct((NX, 2, 32, WIDTH), jnp.bfloat16)
    tokens = pltpu.VMEM((TOK, WIDTH), jnp.bfloat16)
    return pl.pallas_call(
        layer_kernel,
        out_shape=(piece, piece, jax.ShapeDtypeStruct((TOK, UNITS), jnp.bfloat16)),
        in_specs=[SMEM, VMEM, VMEM, HBM, HBM, HBM, HBM],
        out_specs=(VMEM, VMEM, VMEM),
        scratch_shapes=[
            tokens,
            tokens,
            tokens,
            pltpu.VMEM((WIDTH, 3 * UNITS), jnp.bfloat16),
            pltpu.SemaphoreType.DMA((2, 8, 8)),
            pltpu.SemaphoreType.DMA((3,)),
        ],
        compiler_params=pltpu.CompilerParams(vmem_limit_bytes=58 * 1024 * 1024),
        cost_estimate=pl.CostEstimate(
            flops=6_000_000_000, transcendentals=0, bytes_accessed=12_000_000
        ),
        name="layer",
    )(strides, taps, bias, x_early, x_late, cot, w)


def gradient_kernel(stride_ref, cot_t_ref, hidden_ref, grad_ref):
    outer = stride_ref[0]
    inner = stride_ref[1]
    for k in range(8):
        part = jnp.dot(
            cot_t_ref[k * 256 : (k + 1) * 256, :],
            hidden_ref[...],
            preferred_element_type=jnp.float32,
        ).astype(jnp.bfloat16)
        for j in range(8):
            at = pl.multiple_of((k * outer + j * inner) * 32, 32)
            grad_ref[pl.ds(at, 32), :] = part[j * 32 : (j + 1) * 32, :]


def gradient(strides, cot_t, hidden):
    return pl.pallas_call(
        gradient_kernel,
        out_shape=jax.ShapeDtypeStruct((WIDTH, UNITS), jnp.bfloat16),
        in_specs=[SMEM, VMEM, VMEM],
        out_specs=VMEM,
        compiler_params=pltpu.CompilerParams(vmem_limit_bytes=16 * 1024 * 1024),
        cost_estimate=pl.CostEstimate(
            flops=1_000_000_000, transcendentals=0, bytes_accessed=4_000_000
        ),
        name="gradient",
    )(strides, cot_t, hidden)


def assemble_kernel(place_ref, mine_ref, other_ref, y_ref, dx_ref, sems):
    x = place_ref[0]
    core = place_ref[1]
    copies = []
    for who, ref in enumerate((mine_ref, other_ref)):
        half = core if who == 0 else 1 - core
        for d in range(NX):
            at = pl.multiple_of(half * 128 + lax.rem(x + NX - d, NX) * 32, 32)
            for k, out in enumerate((y_ref, dx_ref)):
                copies.append(
                    pltpu.make_async_copy(
                        ref.at[d, k], out.at[pl.ds(at, 32)], sems.at[who, d, k]
                    )
                )
    for c in copies:
        c.start()
    for c in copies:
        c.wait()


def assemble(where, mine, other):
    out = jax.ShapeDtypeStruct((TOK, WIDTH), jnp.bfloat16)
    return pl.pallas_call(
        assemble_kernel,
        out_shape=(out, out),
        in_specs=[SMEM, VMEM, VMEM],
        out_specs=(HBM, HBM),
        scratch_shapes=[pltpu.SemaphoreType.DMA((2, NX, 2))],
        compiler_params=pltpu.CompilerParams(vmem_limit_bytes=4 * 1024 * 1024),
        name="assemble",
    )(where, mine, other)


def exchanged(value):
    return lax.ppermute(value, "c", [(0, 1), (1, 0)])


def moved(value, steps):
    return lax.ppermute(value, "x", [(i, (i + steps) % NX) for i in range(NX)])


def f32_sum(pieces):
    return pieces.astype(jnp.float32).sum(axis=0).astype(jnp.bfloat16)


def shards(x_late, x_early, cotangent, w_gate, w_up, w_down, conv_taps, conv_bias, grad_down):
    core = lax.axis_index("c")
    x = lax.axis_index("x")
    offset = lax.axis_index(TP) * UNITS
    taps = lax.dynamic_slice_in_dim(conv_taps, offset, UNITS, 1)
    bias = lax.dynamic_slice_in_dim(conv_bias, offset, UNITS, 0)[None]
    mine = jnp.concatenate([w_gate, w_up, w_down.T], axis=1)
    near = lax.all_to_all(
        jnp.broadcast_to(mine[None], (8,) + mine.shape), AXES, 0, 0,
        tiled=True, axis_index_groups=FIRST,
    )
    w = lax.all_gather(near, AXES, axis_index_groups=SECOND)
    strides = jnp.stack([8 - 7 * core, 1 + 7 * core]).astype(jnp.int32)
    keep, give, hidden = layer(strides, taps, bias, x_early, x_late, cotangent, w)
    grad_part = gradient(strides, cotangent.T, hidden)

    grad = lax.all_to_all(
        grad_part.reshape(8, 256, UNITS), AXES, 0, 0, tiled=True, axis_index_groups=SECOND
    )
    grad = f32_sum(grad).reshape(8, 32, UNITS)
    grad = lax.all_to_all(grad, AXES, 0, 0, tiled=True, axis_index_groups=FIRST)
    grad_down_out = grad_down + grad.astype(jnp.float32).sum(axis=0).T

    got = exchanged(give)

    def chip_piece(at):
        left = lax.dynamic_index_in_dim(keep, at, 0, keepdims=False)
        right = lax.dynamic_index_in_dim(got, at, 0, keepdims=False)
        return left.astype(jnp.float32) + right.astype(jnp.float32)

    total = chip_piece(x)
    for d in range(1, NX):
        sent = chip_piece(lax.rem(x + d, NX)).astype(jnp.bfloat16)
        total = total + moved(sent, d).astype(jnp.float32)
    total = total.astype(jnp.bfloat16)
    mine = jnp.stack([total] + [moved(total, d) for d in range(1, NX)])
    other = exchanged(mine)
    where = jnp.stack([x, core]).astype(jnp.int32)
    y_late, dx_early = assemble(where, mine, other)
    return (y_late, dx_early, grad_down_out)


def solution(mesh):
    torus = Mesh(mesh.devices.reshape(NZ, NY, NX, NC), AXES)
    return jax.shard_map(
        shards,
        mesh=torus,
        in_specs=(
            P(FS, None),
            P(FS, None),
            P(FS, None),
            P(FS, TP),
            P(FS, TP),
            P(TP, FS),
            P(),
            P(),
            P(TP, FS),
        ),
        out_specs=(P(FS, None), P(FS, None), P(TP, FS)),
        check_vma=False,
    )
```

```python
import jax
import jax.numpy as jnp
from jax import lax
from jax.experimental import pallas as pl
from jax.experimental.pallas import tpu as pltpu
from jax.sharding import Mesh
from jax.sharding import PartitionSpec as P

AXES = ("z", "y", "x", "c")
FS = ("z", "y")
TP = ("x", "c")
NZ, NY, NX, NC = 8, 8, 4, 2
UNITS = 512
TOK = 256
WIDTH = 2048


def place(z, y, x, c):
    return ((z * NY + y) * NX + x) * NC + c


def split_groups(core_along_y):
    groups = []
    for x in range(NX):
        for k in range(8):
            groups.append([place(k, y, x, core_along_y) for y in range(NY)])
            groups.append([place(z, k, x, 1 - core_along_y) for z in range(NZ)])
    return groups


FIRST = split_groups(0)
SECOND = split_groups(1)


def ring_pairs(step):
    pairs = []
    for z in range(NZ):
        for y in range(NY):
            for x in range(NX):
                pairs.append((place(z, y, x, 0), place((z + step) % NZ, y, x, 0)))
                pairs.append((place(z, y, x, 1), place(z, (y + step) % NY, x, 1)))
    return pairs


UP = ring_pairs(1)
DOWN = ring_pairs(-1)


def ring_gather(own):
    up = down = own
    chunks = [own]
    for _ in range(3):
        up = lax.ppermute(up, AXES, UP)
        down = lax.ppermute(down, AXES, DOWN)
        chunks += [up, down]
    chunks.append(lax.ppermute(up[:4], AXES, UP))
    chunks.append(lax.ppermute(down[4:], AXES, DOWN))
    return chunks


def contract_last(left, right):
    return lax.dot_general(
        left, right, (((1,), (1,)), ((), ())), preferred_element_type=jnp.float32
    )


def shift_later(field, steps):
    row = lax.broadcasted_iota(jnp.int32, field.shape, 0)
    return jnp.where(row >= steps, pltpu.roll(field, steps, 0), 0.0)


def shift_earlier(field, steps):
    rows = field.shape[0]
    row = lax.broadcasted_iota(jnp.int32, field.shape, 0)
    return jnp.where(row < rows - steps, pltpu.roll(field, rows - steps, 0), 0.0)


def hidden_parts(x, w_ref, taps_ref, bias_ref):
    t0, t1, t2 = taps_ref[0:1, :], taps_ref[1:2, :], taps_ref[2:3, :]
    gate = jnp.dot(x, w_ref[:, 0:UNITS], preferred_element_type=jnp.float32)
    gate = gate.astype(jnp.bfloat16).astype(jnp.float32)
    up = jnp.dot(x, w_ref[:, UNITS : 2 * UNITS], preferred_element_type=jnp.float32)
    conv = bias_ref[0:1, :] + t2 * gate + t1 * shift_later(gate, 1) + t0 * shift_later(gate, 2)
    return conv, up


def sigmoid(v):
    return 1.0 / (1.0 + jnp.exp(-v))


def layer_kernel(
    stride_ref, taps_ref, bias_ref, xe_hbm, xl_hbm, cot_hbm, *refs
):
    chunks = refs[:9]
    keep_ref, give_ref, hidden_ref, xe_ref, xl_ref, cot_ref, w_ref, w_sems, x_sems = refs[9:]
    spot = stride_ref[2]
    outer = stride_ref[0]
    inner = stride_ref[1]
    south = outer == 8

    def w_copy(p, j, part):
        source = chunks[8] if p == 7 and j >= 4 else chunks[p]
        row = j - 4 if p == 7 and j >= 4 else j
        at = lax.rem(spot + (0, 7, 1, 6, 2, 5, 3, 4)[p], 8)
        at = pl.multiple_of((at * outer + j * inner) * 32, 32)
        cols = pl.ds(0, 2 * UNITS) if part == 0 else pl.ds(2 * UNITS, UNITS)
        return pltpu.make_async_copy(
            source.at[row, :, cols], w_ref.at[pl.ds(at, 32), cols], w_sems.at[part, p, j]
        )

    blocks = [(p, j) for p in range(8) for j in range(8)]
    xe_copy = pltpu.make_async_copy(xe_hbm, xe_ref, x_sems.at[0])
    cot_copy = pltpu.make_async_copy(cot_hbm, cot_ref, x_sems.at[1])
    xl_copy = pltpu.make_async_copy(xl_hbm, xl_ref, x_sems.at[2])
    xe_copy.start()
    for p, j in blocks:
        w_copy(p, j, 0).start()
    cot_copy.start()
    for p, j in blocks:
        w_copy(p, j, 1).start()
    xl_copy.start()

    def put(value, at):
        value = value.astype(jnp.bfloat16)

        @pl.when(south)
        def _():
            for k in range(NX):
                keep_ref[k, at] = value[k * 32 : (k + 1) * 32]
                give_ref[k, at] = value[128 + k * 32 : 128 + (k + 1) * 32]

        @pl.when(jnp.logical_not(south))
        def _():
            for k in range(NX):
                give_ref[k, at] = value[k * 32 : (k + 1) * 32]
                keep_ref[k, at] = value[128 + k * 32 : 128 + (k + 1) * 32]

    t0, t1, t2 = taps_ref[0:1, :], taps_ref[1:2, :], taps_ref[2:3, :]
    xe_copy.wait()
    for p, j in blocks:
        w_copy(p, j, 0).wait()
    conv, up = hidden_parts(xe_ref[...], w_ref, taps_ref, bias_ref)
    sig = sigmoid(conv)
    act = conv * sig
    hidden_ref[...] = (act * up).astype(jnp.bfloat16)
    slope = up * sig * (1.0 + conv * (1.0 - sig))
    cot_copy.wait()
    for p, j in blocks:
        w_copy(p, j, 1).wait()
    w_down = w_ref[:, 2 * UNITS : 3 * UNITS]
    dhidden = jnp.dot(cot_ref[...], w_down, preferred_element_type=jnp.float32)
    dup = (dhidden * act).astype(jnp.bfloat16)
    dconv = dhidden * slope
    dgate = t2 * dconv + t1 * shift_earlier(dconv, 1) + t0 * shift_earlier(dconv, 2)
    dgate = dgate.astype(jnp.bfloat16)
    put(
        contract_last(dup, w_ref[:, UNITS : 2 * UNITS]) + contract_last(dgate, w_ref[:, 0:UNITS]),
        1,
    )
    xl_copy.wait()
    late, late_up = hidden_parts(xl_ref[...], w_ref, taps_ref, bias_ref)
    put(contract_last((late * sigmoid(late) * late_up).astype(jnp.bfloat16), w_down), 0)


VMEM = pl.BlockSpec(memory_space=pltpu.VMEM)
SMEM = pl.BlockSpec(memory_space=pltpu.SMEM)
HBM = pl.BlockSpec(memory_space=pltpu.HBM)


def layer(strides, taps, bias, x_early, x_late, cot, chunks):
    piece = jax.ShapeDtypeStruct((NX, 2, 32, WIDTH), jnp.bfloat16)
    tokens = pltpu.VMEM((TOK, WIDTH), jnp.bfloat16)
    return pl.pallas_call(
        layer_kernel,
        out_shape=(piece, piece, jax.ShapeDtypeStruct((TOK, UNITS), jnp.bfloat16)),
        in_specs=[SMEM, VMEM, VMEM, HBM, HBM, HBM] + [HBM] * 9,
        out_specs=(VMEM, VMEM, VMEM),
        scratch_shapes=[
            tokens,
            tokens,
            tokens,
            pltpu.VMEM((WIDTH, 3 * UNITS), jnp.bfloat16),
            pltpu.SemaphoreType.DMA((2, 8, 8)),
            pltpu.SemaphoreType.DMA((3,)),
        ],
        compiler_params=pltpu.CompilerParams(vmem_limit_bytes=58 * 1024 * 1024),
        cost_estimate=pl.CostEstimate(
            flops=6_000_000_000, transcendentals=0, bytes_accessed=12_000_000
        ),
        name="layer",
    )(strides, taps, bias, x_early, x_late, cot, *chunks)


def gradient_kernel(stride_ref, cot_t_ref, hidden_ref, grad_ref):
    outer = stride_ref[0]
    inner = stride_ref[1]
    for k in range(8):
        part = jnp.dot(
            cot_t_ref[k * 256 : (k + 1) * 256, :],
            hidden_ref[...],
            preferred_element_type=jnp.float32,
        ).astype(jnp.bfloat16)
        for j in range(8):
            at = pl.multiple_of((k * outer + j * inner) * 32, 32)
            grad_ref[pl.ds(at, 32), :] = part[j * 32 : (j + 1) * 32, :]


def gradient(strides, cot_t, hidden):
    return pl.pallas_call(
        gradient_kernel,
        out_shape=jax.ShapeDtypeStruct((WIDTH, UNITS), jnp.bfloat16),
        in_specs=[SMEM, VMEM, VMEM],
        out_specs=VMEM,
        compiler_params=pltpu.CompilerParams(vmem_limit_bytes=16 * 1024 * 1024),
        cost_estimate=pl.CostEstimate(
            flops=1_000_000_000, transcendentals=0, bytes_accessed=4_000_000
        ),
        name="gradient",
    )(strides, cot_t, hidden)


def assemble_kernel(place_ref, mine_ref, other_ref, y_ref, dx_ref, sems):
    x = place_ref[0]
    core = place_ref[1]
    copies = []
    for who, ref in enumerate((mine_ref, other_ref)):
        half = core if who == 0 else 1 - core
        for d in range(NX):
            at = pl.multiple_of(half * 128 + lax.rem(x + NX - d, NX) * 32, 32)
            for k, out in enumerate((y_ref, dx_ref)):
                copies.append(
                    pltpu.make_async_copy(
                        ref.at[d, k], out.at[pl.ds(at, 32)], sems.at[who, d, k]
                    )
                )
    for c in copies:
        c.start()
    for c in copies:
        c.wait()


def assemble(where, mine, other):
    out = jax.ShapeDtypeStruct((TOK, WIDTH), jnp.bfloat16)
    return pl.pallas_call(
        assemble_kernel,
        out_shape=(out, out),
        in_specs=[SMEM, VMEM, VMEM],
        out_specs=(HBM, HBM),
        scratch_shapes=[pltpu.SemaphoreType.DMA((2, NX, 2))],
        compiler_params=pltpu.CompilerParams(vmem_limit_bytes=4 * 1024 * 1024),
        name="assemble",
    )(where, mine, other)


def exchanged(value):
    return lax.ppermute(value, "c", [(0, 1), (1, 0)])


def moved(value, steps):
    return lax.ppermute(value, "x", [(i, (i + steps) % NX) for i in range(NX)])


def f32_sum(pieces):
    return pieces.astype(jnp.float32).sum(axis=0).astype(jnp.bfloat16)


def shards(x_late, x_early, cotangent, w_gate, w_up, w_down, conv_taps, conv_bias, grad_down):
    core = lax.axis_index("c")
    x = lax.axis_index("x")
    offset = lax.axis_index(TP) * UNITS
    taps = lax.dynamic_slice_in_dim(conv_taps, offset, UNITS, 1)
    bias = lax.dynamic_slice_in_dim(conv_bias, offset, UNITS, 0)[None]
    mine = jnp.concatenate([w_gate, w_up, w_down.T], axis=1)
    near = lax.all_to_all(
        jnp.broadcast_to(mine[None], (8,) + mine.shape), AXES, 0, 0,
        tiled=True, axis_index_groups=FIRST,
    )
    chunks = ring_gather(near)
    spot = jnp.where(core == 0, lax.axis_index("z"), lax.axis_index("y"))
    strides = jnp.stack([8 - 7 * core, 1 + 7 * core, spot]).astype(jnp.int32)
    keep, give, hidden = layer(strides, taps, bias, x_early, x_late, cotangent, chunks)
    grad_part = gradient(strides, cotangent.T, hidden)
    grad = lax.all_to_all(
        grad_part.reshape(8, 256, UNITS), AXES, 0, 0, tiled=True, axis_index_groups=SECOND
    )
    grad = f32_sum(grad).reshape(8, 32, UNITS)
    grad = lax.all_to_all(grad, AXES, 0, 0, tiled=True, axis_index_groups=FIRST)
    grad_down_out = grad_down + grad.astype(jnp.float32).sum(axis=0).T

    got = exchanged(give)

    def chip_piece(at):
        left = lax.dynamic_index_in_dim(keep, at, 0, keepdims=False)
        right = lax.dynamic_index_in_dim(got, at, 0, keepdims=False)
        return left.astype(jnp.float32) + right.astype(jnp.float32)

    total = chip_piece(x)
    for d in range(1, NX):
        sent = chip_piece(lax.rem(x + d, NX)).astype(jnp.bfloat16)
        total = total + moved(sent, d).astype(jnp.float32)
    total = total.astype(jnp.bfloat16)
    spread = [moved(total, d) for d in range(1, NX)]
    mine = jnp.stack([total] + spread)
    other = exchanged(mine)
    where = jnp.stack([x, core]).astype(jnp.int32)
    y_late, dx_early = assemble(where, mine, other)
    return (y_late, dx_early, grad_down_out)


def solution(mesh):
    torus = Mesh(mesh.devices.reshape(NZ, NY, NX, NC), AXES)
    return jax.shard_map(
        shards,
        mesh=torus,
        in_specs=(
            P(FS, None),
            P(FS, None),
            P(FS, None),
            P(FS, TP),
            P(FS, TP),
            P(TP, FS),
            P(),
            P(),
            P(TP, FS),
        ),
        out_specs=(P(FS, None), P(FS, None), P(TP, FS)),
        check_vma=False,
    )
```

```python
import jax
import jax.numpy as jnp
from jax import lax
from jax.experimental import pallas as pl
from jax.experimental.pallas import tpu as pltpu
from jax.sharding import Mesh
from jax.sharding import PartitionSpec as P

AXES = ("z", "y", "x", "c")
FS = ("z", "y")
TP = ("x", "c")
NZ, NY, NX, NC = 8, 8, 4, 2
UNITS = 512
TOK = 256
WIDTH = 2048


def place(z, y, x, c):
    return ((z * NY + y) * NX + x) * NC + c


def split_groups(core_along_y):
    groups = []
    for x in range(NX):
        for k in range(8):
            groups.append([place(k, y, x, core_along_y) for y in range(NY)])
            groups.append([place(z, k, x, 1 - core_along_y) for z in range(NZ)])
    return groups


FIRST = split_groups(0)
SECOND = split_groups(1)


def contract_last(left, right):
    return lax.dot_general(
        left, right, (((1,), (1,)), ((), ())), preferred_element_type=jnp.float32
    )


def shift_later(field, steps):
    row = lax.broadcasted_iota(jnp.int32, field.shape, 0)
    return jnp.where(row >= steps, pltpu.roll(field, steps, 0), 0.0)


def shift_earlier(field, steps):
    rows = field.shape[0]
    row = lax.broadcasted_iota(jnp.int32, field.shape, 0)
    return jnp.where(row < rows - steps, pltpu.roll(field, rows - steps, 0), 0.0)


def hidden_parts(x, w_ref, taps_ref, bias_ref):
    t0, t1, t2 = taps_ref[0:1, :], taps_ref[1:2, :], taps_ref[2:3, :]
    gate = jnp.dot(x, w_ref[:, 0:UNITS], preferred_element_type=jnp.float32)
    gate = gate.astype(jnp.bfloat16).astype(jnp.float32)
    up = jnp.dot(x, w_ref[:, UNITS : 2 * UNITS], preferred_element_type=jnp.float32)
    conv = bias_ref[0:1, :] + t2 * gate + t1 * shift_later(gate, 1) + t0 * shift_later(gate, 2)
    return conv, up


def sigmoid(v):
    return 1.0 / (1.0 + jnp.exp(-v))


def layer_kernel(
    stride_ref, taps_ref, bias_ref, xe_hbm, xl_hbm, cot_hbm, w_hbm,
    keep_ref, give_ref, hidden_ref,
    xe_ref, xl_ref, cot_ref, w_ref, w_sems, x_sems,
):
    outer = stride_ref[0]
    inner = stride_ref[1]
    south = outer == 8

    def w_copy(p, j, part):
        at = pl.multiple_of((p * outer + j * inner) * 32, 32)
        cols = pl.ds(0, 2 * UNITS) if part == 0 else pl.ds(2 * UNITS, UNITS)
        return pltpu.make_async_copy(
            w_hbm.at[p, j, :, cols], w_ref.at[pl.ds(at, 32), cols], w_sems.at[part, p, j]
        )

    blocks = [(p, j) for p in range(8) for j in range(8)]
    xe_copy = pltpu.make_async_copy(xe_hbm, xe_ref, x_sems.at[0])
    cot_copy = pltpu.make_async_copy(cot_hbm, cot_ref, x_sems.at[1])
    xl_copy = pltpu.make_async_copy(xl_hbm, xl_ref, x_sems.at[2])
    xe_copy.start()
    for p, j in blocks:
        w_copy(p, j, 0).start()
    cot_copy.start()
    for p, j in blocks:
        w_copy(p, j, 1).start()
    xl_copy.start()

    def put(value, at):
        value = value.astype(jnp.bfloat16)

        @pl.when(south)
        def _():
            for k in range(NX):
                keep_ref[k, at] = value[k * 32 : (k + 1) * 32]
                give_ref[k, at] = value[128 + k * 32 : 128 + (k + 1) * 32]

        @pl.when(jnp.logical_not(south))
        def _():
            for k in range(NX):
                give_ref[k, at] = value[k * 32 : (k + 1) * 32]
                keep_ref[k, at] = value[128 + k * 32 : 128 + (k + 1) * 32]

    t0, t1, t2 = taps_ref[0:1, :], taps_ref[1:2, :], taps_ref[2:3, :]
    xe_copy.wait()
    for p, j in blocks:
        w_copy(p, j, 0).wait()
    conv, up = hidden_parts(xe_ref[...], w_ref, taps_ref, bias_ref)
    sig = sigmoid(conv)
    act = conv * sig
    hidden_ref[...] = (act * up).astype(jnp.bfloat16)
    slope = up * sig * (1.0 + conv * (1.0 - sig))
    cot_copy.wait()
    for p, j in blocks:
        w_copy(p, j, 1).wait()
    w_down = w_ref[:, 2 * UNITS : 3 * UNITS]
    dhidden = jnp.dot(cot_ref[...], w_down, preferred_element_type=jnp.float32)
    dup = (dhidden * act).astype(jnp.bfloat16)
    dconv = dhidden * slope
    dgate = t2 * dconv + t1 * shift_earlier(dconv, 1) + t0 * shift_earlier(dconv, 2)
    dgate = dgate.astype(jnp.bfloat16)
    put(
        contract_last(dup, w_ref[:, UNITS : 2 * UNITS]) + contract_last(dgate, w_ref[:, 0:UNITS]),
        1,
    )
    xl_copy.wait()
    late, late_up = hidden_parts(xl_ref[...], w_ref, taps_ref, bias_ref)
    put(contract_last((late * sigmoid(late) * late_up).astype(jnp.bfloat16), w_down), 0)


VMEM = pl.BlockSpec(memory_space=pltpu.VMEM)
SMEM = pl.BlockSpec(memory_space=pltpu.SMEM)
HBM = pl.BlockSpec(memory_space=pltpu.HBM)


def layer(strides, taps, bias, x_early, x_late, cot, w):
    piece = jax.ShapeDtypeStruct((NX, 2, 32, WIDTH), jnp.bfloat16)
    tokens = pltpu.VMEM((TOK, WIDTH), jnp.bfloat16)
    return pl.pallas_call(
        layer_kernel,
        out_shape=(piece, piece, jax.ShapeDtypeStruct((TOK, UNITS), jnp.bfloat16)),
        in_specs=[SMEM, VMEM, VMEM, HBM, HBM, HBM, HBM],
        out_specs=(VMEM, VMEM, VMEM),
        scratch_shapes=[
            tokens,
            tokens,
            tokens,
            pltpu.VMEM((WIDTH, 3 * UNITS), jnp.bfloat16),
            pltpu.SemaphoreType.DMA((2, 8, 8)),
            pltpu.SemaphoreType.DMA((3,)),
        ],
        compiler_params=pltpu.CompilerParams(vmem_limit_bytes=58 * 1024 * 1024),
        cost_estimate=pl.CostEstimate(
            flops=6_000_000_000, transcendentals=0, bytes_accessed=12_000_000
        ),
        name="layer",
    )(strides, taps, bias, x_early, x_late, cot, w)


def gradient_kernel(stride_ref, cot_t_ref, hidden_ref, grad_ref):
    outer = stride_ref[0]
    inner = stride_ref[1]
    for k in range(8):
        part = jnp.dot(
            cot_t_ref[k * 256 : (k + 1) * 256, :],
            hidden_ref[...],
            preferred_element_type=jnp.float32,
        ).astype(jnp.bfloat16)
        for j in range(8):
            at = pl.multiple_of((k * outer + j * inner) * 32, 32)
            grad_ref[pl.ds(at, 32), :] = part[j * 32 : (j + 1) * 32, :]


def gradient(strides, cot_t, hidden):
    return pl.pallas_call(
        gradient_kernel,
        out_shape=jax.ShapeDtypeStruct((WIDTH, UNITS), jnp.bfloat16),
        in_specs=[SMEM, VMEM, VMEM],
        out_specs=VMEM,
        compiler_params=pltpu.CompilerParams(vmem_limit_bytes=16 * 1024 * 1024),
        cost_estimate=pl.CostEstimate(
            flops=1_000_000_000, transcendentals=0, bytes_accessed=4_000_000
        ),
        name="gradient",
    )(strides, cot_t, hidden)


def assemble_kernel(place_ref, mine_ref, other_ref, y_ref, dx_ref, sems):
    x = place_ref[0]
    core = place_ref[1]
    copies = []
    for who, ref in enumerate((mine_ref, other_ref)):
        half = core if who == 0 else 1 - core
        for d in range(NX):
            at = pl.multiple_of(half * 128 + lax.rem(x + NX - d, NX) * 32, 32)
            for k, out in enumerate((y_ref, dx_ref)):
                copies.append(
                    pltpu.make_async_copy(
                        ref.at[d, k], out.at[pl.ds(at, 32)], sems.at[who, d, k]
                    )
                )
    for c in copies:
        c.start()
    for c in copies:
        c.wait()


def assemble(where, mine, other):
    out = jax.ShapeDtypeStruct((TOK, WIDTH), jnp.bfloat16)
    return pl.pallas_call(
        assemble_kernel,
        out_shape=(out, out),
        in_specs=[SMEM, VMEM, VMEM],
        out_specs=(HBM, HBM),
        scratch_shapes=[pltpu.SemaphoreType.DMA((2, NX, 2))],
        compiler_params=pltpu.CompilerParams(vmem_limit_bytes=4 * 1024 * 1024),
        name="assemble",
    )(where, mine, other)


def exchanged(value):
    return lax.ppermute(value, "c", [(0, 1), (1, 0)])


def moved(value, steps):
    return lax.ppermute(value, "x", [(i, (i + steps) % NX) for i in range(NX)])


def f32_sum(pieces):
    return pieces.astype(jnp.float32).sum(axis=0).astype(jnp.bfloat16)


def shards(x_late, x_early, cotangent, w_gate, w_up, w_down, conv_taps, conv_bias, grad_down):
    core = lax.axis_index("c")
    x = lax.axis_index("x")
    offset = lax.axis_index(TP) * UNITS
    taps = lax.dynamic_slice_in_dim(conv_taps, offset, UNITS, 1)
    bias = lax.dynamic_slice_in_dim(conv_bias, offset, UNITS, 0)[None]
    mine = jnp.concatenate([w_gate, w_up, w_down.T], axis=1)
    near = lax.all_to_all(
        jnp.broadcast_to(mine[None], (8,) + mine.shape), AXES, 0, 0,
        tiled=True, axis_index_groups=FIRST,
    )
    w = lax.all_gather(near, AXES, axis_index_groups=SECOND)
    strides = jnp.stack([8 - 7 * core, 1 + 7 * core]).astype(jnp.int32)
    keep, give, hidden = layer(strides, taps, bias, x_early, x_late, cotangent, w)
    grad_part = gradient(strides, cotangent.T, hidden)
    grad = lax.all_to_all(
        grad_part.reshape(8, 256, UNITS), AXES, 0, 0, tiled=True, axis_index_groups=SECOND
    )
    grad = f32_sum(grad).reshape(8, 32, UNITS)
    grad = lax.all_to_all(grad, AXES, 0, 0, tiled=True, axis_index_groups=FIRST)
    grad_down_out = grad_down + grad.astype(jnp.float32).sum(axis=0).T

    got = exchanged(give)

    def chip_piece(at):
        left = lax.dynamic_index_in_dim(keep, at, 0, keepdims=False)
        right = lax.dynamic_index_in_dim(got, at, 0, keepdims=False)
        return left.astype(jnp.float32) + right.astype(jnp.float32)

    total = chip_piece(x)
    for d in range(1, NX):
        sent = chip_piece(lax.rem(x + d, NX)).astype(jnp.bfloat16)
        arrived = moved(sent, d)
        total = total + arrived.astype(jnp.float32)
    total = total.astype(jnp.bfloat16)
    spread = [moved(total, d) for d in range(1, NX)]
    mine = jnp.stack([total] + spread)
    other = exchanged(mine)
    where = jnp.stack([x, core]).astype(jnp.int32)
    y_late, dx_early = assemble(where, mine, other)
    return (y_late, dx_early, grad_down_out)


def solution(mesh):
    torus = Mesh(mesh.devices.reshape(NZ, NY, NX, NC), AXES)
    return jax.shard_map(
        shards,
        mesh=torus,
        in_specs=(
            P(FS, None),
            P(FS, None),
            P(FS, None),
            P(FS, TP),
            P(FS, TP),
            P(TP, FS),
            P(),
            P(),
            P(TP, FS),
        ),
        out_specs=(P(FS, None), P(FS, None), P(TP, FS)),
        check_vma=False,
    )
```

```python
import jax
import jax.numpy as jnp
from jax import lax
from jax.experimental import pallas as pl
from jax.experimental.pallas import tpu as pltpu
from jax.sharding import Mesh
from jax.sharding import PartitionSpec as P

AXES = ("z", "y", "x", "c")
FS = ("z", "y")
TP = ("x", "c")
NZ, NY, NX, NC = 8, 8, 4, 2
UNITS = 512
TOK = 256
WIDTH = 2048


def place(z, y, x, c):
    return ((z * NY + y) * NX + x) * NC + c


def split_groups(core_along_y):
    groups = []
    for x in range(NX):
        for k in range(8):
            groups.append([place(k, y, x, core_along_y) for y in range(NY)])
            groups.append([place(z, k, x, 1 - core_along_y) for z in range(NZ)])
    return groups


FIRST = split_groups(0)
SECOND = split_groups(1)


def contract_last(left, right):
    return lax.dot_general(
        left, right, (((1,), (1,)), ((), ())), preferred_element_type=jnp.float32
    )


def shift_later(field, steps):
    row = lax.broadcasted_iota(jnp.int32, field.shape, 0)
    return jnp.where(row >= steps, pltpu.roll(field, steps, 0), 0.0)


def shift_earlier(field, steps):
    rows = field.shape[0]
    row = lax.broadcasted_iota(jnp.int32, field.shape, 0)
    return jnp.where(row < rows - steps, pltpu.roll(field, rows - steps, 0), 0.0)


def conv_and_up(both, taps_ref, bias_ref):
    t0, t1, t2 = taps_ref[0:1, :], taps_ref[1:2, :], taps_ref[2:3, :]
    gate = both[:, 0:UNITS].astype(jnp.bfloat16).astype(jnp.float32)
    up = both[:, UNITS : 2 * UNITS]
    conv = bias_ref[0:1, :] + t2 * gate + t1 * shift_later(gate, 1) + t0 * shift_later(gate, 2)
    return conv, up


def sigmoid(v):
    return 1.0 / (1.0 + jnp.exp(-v))


def layer_kernel(
    stride_ref, taps_ref, bias_ref, xe_hbm, xl_hbm, cot_ref, w_hbm,
    keep_ref, give_ref, hidden_ref, w_ref, xe_ref, xl_ref, w_sems, x_sems,
):
    south = stride_ref[0] == 8

    def w_copy(a, m, part):
        p = jnp.where(south, a, m)
        j = jnp.where(south, m, a)
        rows = pl.ds((a * 8 + m) * 32, 32)
        cols = pl.ds(0, 2 * UNITS) if part == 0 else pl.ds(2 * UNITS, UNITS)
        return pltpu.make_async_copy(
            w_hbm.at[p, j, :, cols], w_ref.at[rows, cols], w_sems.at[part, a, m]
        )

    blocks = [(a, m) for a in range(8) for m in range(8)]
    xl_copy = pltpu.make_async_copy(xl_hbm, xl_ref, x_sems.at[4])

    def xe_copy(k):
        cols = pl.ds(k * 512, 512)
        return pltpu.make_async_copy(xe_hbm.at[:, cols], xe_ref.at[:, cols], x_sems.at[k])

    for a, m in blocks:
        if a % 2 == 0 and m == 0:
            xe_copy(a // 2).start()
        w_copy(a, m, 0).start()
    xl_copy.start()
    for a, m in blocks:
        w_copy(a, m, 1).start()

    def put(value, at):
        value = value.astype(jnp.bfloat16)

        @pl.when(south)
        def _():
            for k in range(NX):
                keep_ref[k, at] = value[k * 32 : (k + 1) * 32]
                give_ref[k, at] = value[128 + k * 32 : 128 + (k + 1) * 32]

        @pl.when(jnp.logical_not(south))
        def _():
            for k in range(NX):
                give_ref[k, at] = value[k * 32 : (k + 1) * 32]
                keep_ref[k, at] = value[128 + k * 32 : 128 + (k + 1) * 32]

    t0, t1, t2 = taps_ref[0:1, :], taps_ref[1:2, :], taps_ref[2:3, :]
    both = jnp.zeros((TOK, 2 * UNITS), jnp.float32)
    for k in range(4):
        xe_copy(k).wait()
        for a in (2 * k, 2 * k + 1):
            for m in range(8):
                w_copy(a, m, 0).wait()
        both = both + jnp.dot(
            xe_ref[:, k * 512 : (k + 1) * 512],
            w_ref[k * 512 : (k + 1) * 512, 0 : 2 * UNITS],
            preferred_element_type=jnp.float32,
        )
    conv, up = conv_and_up(both, taps_ref, bias_ref)
    sig = sigmoid(conv)
    act = conv * sig
    hidden_ref[...] = (act * up).astype(jnp.bfloat16)
    slope = up * sig * (1.0 + conv * (1.0 - sig))
    xl_copy.wait()
    late, late_up = conv_and_up(
        jnp.dot(xl_ref[...], w_ref[:, 0 : 2 * UNITS], preferred_element_type=jnp.float32),
        taps_ref,
        bias_ref,
    )
    late_hidden = (late * sigmoid(late) * late_up).astype(jnp.bfloat16)
    for a, m in blocks:
        w_copy(a, m, 1).wait()
    w_down = w_ref[:, 2 * UNITS : 3 * UNITS]
    dhidden = jnp.dot(cot_ref[...], w_down, preferred_element_type=jnp.float32)
    dup = (dhidden * act).astype(jnp.bfloat16)
    dconv = dhidden * slope
    dgate = t2 * dconv + t1 * shift_earlier(dconv, 1) + t0 * shift_earlier(dconv, 2)
    inward = jnp.concatenate([dgate.astype(jnp.bfloat16), dup], axis=1)
    put(contract_last(inward, w_ref[:, 0 : 2 * UNITS]), 1)
    put(contract_last(late_hidden, w_down), 0)


VMEM = pl.BlockSpec(memory_space=pltpu.VMEM)
SMEM = pl.BlockSpec(memory_space=pltpu.SMEM)
HBM = pl.BlockSpec(memory_space=pltpu.HBM)


def layer(strides, taps, bias, x_early, x_late, cot, w):
    piece = jax.ShapeDtypeStruct((NX, 2, 32, WIDTH), jnp.bfloat16)
    return pl.pallas_call(
        layer_kernel,
        out_shape=(piece, piece, jax.ShapeDtypeStruct((TOK, UNITS), jnp.bfloat16)),
        in_specs=[SMEM, VMEM, VMEM, HBM, HBM, VMEM, HBM],
        out_specs=(VMEM, VMEM, VMEM),
        scratch_shapes=[
            pltpu.VMEM((WIDTH, 3 * UNITS), jnp.bfloat16),
            pltpu.VMEM((TOK, WIDTH), jnp.bfloat16),
            pltpu.VMEM((TOK, WIDTH), jnp.bfloat16),
            pltpu.SemaphoreType.DMA((2, 8, 8)),
            pltpu.SemaphoreType.DMA((5,)),
        ],
        compiler_params=pltpu.CompilerParams(vmem_limit_bytes=36 * 1024 * 1024),
        cost_estimate=pl.CostEstimate(
            flops=6_000_000_000, transcendentals=0, bytes_accessed=12_000_000
        ),
        name="layer",
    )(strides, taps, bias, x_early, x_late, cot, w)


def gradient_kernel(stride_ref, cot_t_ref, hidden_ref, grad_ref):
    outer = stride_ref[0]
    inner = stride_ref[1]
    for k in range(8):
        part = jnp.dot(
            cot_t_ref[k * 256 : (k + 1) * 256, :],
            hidden_ref[...],
            preferred_element_type=jnp.float32,
        ).astype(jnp.bfloat16)
        for j in range(8):
            at = pl.multiple_of((k * outer + j * inner) * 32, 32)
            grad_ref[pl.ds(at, 32), :] = part[j * 32 : (j + 1) * 32, :]


def gradient(strides, cot_t, hidden):
    return pl.pallas_call(
        gradient_kernel,
        out_shape=jax.ShapeDtypeStruct((WIDTH, UNITS), jnp.bfloat16),
        in_specs=[SMEM, VMEM, VMEM],
        out_specs=VMEM,
        compiler_params=pltpu.CompilerParams(vmem_limit_bytes=16 * 1024 * 1024),
        cost_estimate=pl.CostEstimate(
            flops=1_000_000_000, transcendentals=0, bytes_accessed=4_000_000
        ),
        name="gradient",
    )(strides, cot_t, hidden)


def assemble_kernel(place_ref, mine_ref, other_ref, y_ref, dx_ref, sems):
    x = place_ref[0]
    core = place_ref[1]
    copies = []
    for who, ref in enumerate((mine_ref, other_ref)):
        half = core if who == 0 else 1 - core
        for d in range(NX):
            at = pl.multiple_of(half * 128 + lax.rem(x + NX - d, NX) * 32, 32)
            for k, out in enumerate((y_ref, dx_ref)):
                copies.append(
                    pltpu.make_async_copy(
                        ref.at[d, k], out.at[pl.ds(at, 32)], sems.at[who, d, k]
                    )
                )
    for c in copies:
        c.start()
    for c in copies:
        c.wait()


def assemble(where, mine, other):
    out = jax.ShapeDtypeStruct((TOK, WIDTH), jnp.bfloat16)
    return pl.pallas_call(
        assemble_kernel,
        out_shape=(out, out),
        in_specs=[SMEM, VMEM, VMEM],
        out_specs=(HBM, HBM),
        scratch_shapes=[pltpu.SemaphoreType.DMA((2, NX, 2))],
        compiler_params=pltpu.CompilerParams(vmem_limit_bytes=4 * 1024 * 1024),
        name="assemble",
    )(where, mine, other)


def exchanged(value):
    return lax.ppermute(value, "c", [(0, 1), (1, 0)])


def moved(value, steps):
    return lax.ppermute(value, "x", [(i, (i + steps) % NX) for i in range(NX)])


def f32_sum(pieces):
    return pieces.astype(jnp.float32).sum(axis=0).astype(jnp.bfloat16)


def shards(x_late, x_early, cotangent, w_gate, w_up, w_down, conv_taps, conv_bias, grad_down):
    core = lax.axis_index("c")
    x = lax.axis_index("x")
    offset = lax.axis_index(TP) * UNITS
    taps = lax.dynamic_slice_in_dim(conv_taps, offset, UNITS, 1)
    bias = lax.dynamic_slice_in_dim(conv_bias, offset, UNITS, 0)[None]
    mine = jnp.concatenate([w_gate, w_up, w_down.T], axis=1)
    near = lax.all_to_all(
        jnp.broadcast_to(mine[None], (8,) + mine.shape), AXES, 0, 0,
        tiled=True, axis_index_groups=FIRST,
    )
    w = lax.all_gather(near, AXES, axis_index_groups=SECOND)
    w, x_late, x_early = (
        pltpu.with_memory_space_constraint(v, pltpu.HBM) for v in (w, x_late, x_early)
    )
    strides = jnp.stack([8 - 7 * core, 1 + 7 * core]).astype(jnp.int32)
    keep, give, hidden = layer(strides, taps, bias, x_early, x_late, cotangent, w)
    grad_part = gradient(strides, cotangent.T, hidden)
    grad = lax.all_to_all(
        grad_part.reshape(8, 256, UNITS), AXES, 0, 0, tiled=True, axis_index_groups=SECOND
    )
    grad = f32_sum(grad).reshape(8, 32, UNITS)
    grad = lax.all_to_all(grad, AXES, 0, 0, tiled=True, axis_index_groups=FIRST)
    grad_down_out = grad_down + grad.astype(jnp.float32).sum(axis=0).T

    got = exchanged(give)

    def chip_piece(at):
        left = lax.dynamic_index_in_dim(keep, at, 0, keepdims=False)
        right = lax.dynamic_index_in_dim(got, at, 0, keepdims=False)
        return left.astype(jnp.float32) + right.astype(jnp.float32)

    total = chip_piece(x)
    for d in (2, 1, 3):
        sent = chip_piece(lax.rem(x + d, NX)).astype(jnp.bfloat16)
        arrived = moved(sent, d)
        total = total + arrived.astype(jnp.float32)
    total = total.astype(jnp.bfloat16)
    spread = {d: moved(total, d) for d in (2, 1, 3)}
    mine = jnp.stack([total] + [spread[d] for d in range(1, NX)])
    other = exchanged(mine)
    where = jnp.stack([x, core]).astype(jnp.int32)
    y_late, dx_early = assemble(where, mine, other)
    return (y_late, dx_early, grad_down_out)


def solution(mesh):
    torus = Mesh(mesh.devices.reshape(NZ, NY, NX, NC), AXES)
    return jax.shard_map(
        shards,
        mesh=torus,
        in_specs=(
            P(FS, None),
            P(FS, None),
            P(FS, None),
            P(FS, TP),
            P(FS, TP),
            P(TP, FS),
            P(),
            P(),
            P(TP, FS),
        ),
        out_specs=(P(FS, None), P(FS, None), P(TP, FS)),
        check_vma=False,
    )
```

```python
import jax
import jax.numpy as jnp
from jax import lax
from jax.experimental import pallas as pl
from jax.experimental.pallas import tpu as pltpu
from jax.sharding import Mesh
from jax.sharding import PartitionSpec as P

AXES = ("z", "y", "x", "c")
FS = ("z", "y")
TP = ("x", "c")
NZ, NY, NX, NC = 8, 8, 4, 2
UNITS = 512
TOK = 256
WIDTH = 2048


def place(z, y, x, c):
    return ((z * NY + y) * NX + x) * NC + c


def split_groups(core_along_y):
    groups = []
    for x in range(NX):
        for k in range(8):
            groups.append([place(k, y, x, core_along_y) for y in range(NY)])
            groups.append([place(z, k, x, 1 - core_along_y) for z in range(NZ)])
    return groups


FIRST = split_groups(0)
SECOND = split_groups(1)


def contract_last(left, right):
    return lax.dot_general(
        left, right, (((1,), (1,)), ((), ())), preferred_element_type=jnp.float32
    )


def shift_later(field, steps):
    row = lax.broadcasted_iota(jnp.int32, field.shape, 0)
    return jnp.where(row >= steps, pltpu.roll(field, steps, 0), 0.0)


def shift_earlier(field, steps):
    rows = field.shape[0]
    row = lax.broadcasted_iota(jnp.int32, field.shape, 0)
    return jnp.where(row < rows - steps, pltpu.roll(field, rows - steps, 0), 0.0)


def conv_and_up(both, taps_ref, bias_ref):
    t0, t1, t2 = taps_ref[0:1, :], taps_ref[1:2, :], taps_ref[2:3, :]
    gate = both[:, 0:UNITS].astype(jnp.bfloat16).astype(jnp.float32)
    up = both[:, UNITS : 2 * UNITS]
    conv = bias_ref[0:1, :] + t2 * gate + t1 * shift_later(gate, 1) + t0 * shift_later(gate, 2)
    return conv, up


def sigmoid(v):
    return 1.0 / (1.0 + jnp.exp(-v))


def block_copies(south, w_hbm, w_ref, w_sems, x_hbm, x_ref, x_sems):
    def w_copy(a, m, part):
        p = jnp.where(south, a, m)
        j = jnp.where(south, m, a)
        rows = pl.ds((a * 8 + m) * 32, 32)
        cols = pl.ds(0, 2 * UNITS) if part == 0 else pl.ds(2 * UNITS, UNITS)
        return pltpu.make_async_copy(
            w_hbm.at[p, j, :, cols], w_ref.at[rows, cols], w_sems.at[part, a, m]
        )

    def x_copy(k):
        cols = pl.ds(k * 512, 512)
        return pltpu.make_async_copy(x_hbm.at[:, cols], x_ref.at[:, cols], x_sems.at[k])

    return w_copy, x_copy


def start_inward(w_copy, x_copy):
    for k in range(4):
        x_copy(k).start()
        for a in (2 * k, 2 * k + 1):
            for m in range(8):
                w_copy(a, m, 0).start()


def gate_and_up(w_copy, x_copy, w_ref, x_ref):
    both = jnp.zeros((TOK, 2 * UNITS), jnp.float32)
    for k in range(4):
        x_copy(k).wait()
        for a in (2 * k, 2 * k + 1):
            for m in range(8):
                w_copy(a, m, 0).wait()
        both = both + jnp.dot(
            x_ref[:, k * 512 : (k + 1) * 512],
            w_ref[k * 512 : (k + 1) * 512, 0 : 2 * UNITS],
            preferred_element_type=jnp.float32,
        )
    return both


def early_kernel(
    stride_ref, taps_ref, bias_ref, xe_hbm, cot_t_ref, w_hbm,
    grad_ref, act_ref, slope_ref, w_ref, xe_ref, w_sems, x_sems,
):
    outer = stride_ref[0]
    inner = stride_ref[1]
    w_copy, x_copy = block_copies(outer == 8, w_hbm, w_ref, w_sems, xe_hbm, xe_ref, x_sems)
    start_inward(w_copy, x_copy)
    both = gate_and_up(w_copy, x_copy, w_ref, xe_ref)
    conv, up = conv_and_up(both, taps_ref, bias_ref)
    sig = sigmoid(conv)
    act = conv * sig
    act_ref[...] = act
    slope_ref[...] = up * sig * (1.0 + conv * (1.0 - sig))
    hidden = (act * up).astype(jnp.bfloat16)
    for k in range(8):
        part = jnp.dot(
            cot_t_ref[k * 256 : (k + 1) * 256, :], hidden, preferred_element_type=jnp.float32
        ).astype(jnp.bfloat16)
        for j in range(8):
            at = pl.multiple_of((k * outer + j * inner) * 32, 32)
            grad_ref[pl.ds(at, 32), :] = part[j * 32 : (j + 1) * 32, :]


def outputs_kernel(
    stride_ref, taps_ref, bias_ref, xl_hbm, cot_hbm, act_hbm, slope_hbm, w_hbm,
    keep_ref, give_ref, w_ref, xl_ref, cot_ref, act_ref, slope_ref, w_sems, x_sems,
):
    south = stride_ref[0] == 8
    w_copy, x_copy = block_copies(south, w_hbm, w_ref, w_sems, xl_hbm, xl_ref, x_sems)
    start_inward(w_copy, x_copy)
    rest = [
        pltpu.make_async_copy(cot_hbm, cot_ref, x_sems.at[4]),
        pltpu.make_async_copy(act_hbm, act_ref, x_sems.at[5]),
        pltpu.make_async_copy(slope_hbm, slope_ref, x_sems.at[6]),
    ] + [w_copy(a, m, 1) for a in range(8) for m in range(8)]
    for c in rest:
        c.start()

    def put(value, at):
        value = value.astype(jnp.bfloat16)

        @pl.when(south)
        def _():
            for k in range(NX):
                keep_ref[k, at] = value[k * 32 : (k + 1) * 32]
                give_ref[k, at] = value[128 + k * 32 : 128 + (k + 1) * 32]

        @pl.when(jnp.logical_not(south))
        def _():
            for k in range(NX):
                give_ref[k, at] = value[k * 32 : (k + 1) * 32]
                keep_ref[k, at] = value[128 + k * 32 : 128 + (k + 1) * 32]

    t0, t1, t2 = taps_ref[0:1, :], taps_ref[1:2, :], taps_ref[2:3, :]
    both = gate_and_up(w_copy, x_copy, w_ref, xl_ref)
    late, late_up = conv_and_up(both, taps_ref, bias_ref)
    late_hidden = (late * sigmoid(late) * late_up).astype(jnp.bfloat16)
    for c in rest:
        c.wait()
    w_down = w_ref[:, 2 * UNITS : 3 * UNITS]
    put(contract_last(late_hidden, w_down), 0)
    dhidden = jnp.dot(cot_ref[...], w_down, preferred_element_type=jnp.float32)
    dup = (dhidden * act_ref[...]).astype(jnp.bfloat16)
    dconv = dhidden * slope_ref[...]
    dgate = t2 * dconv + t1 * shift_earlier(dconv, 1) + t0 * shift_earlier(dconv, 2)
    inward = jnp.concatenate([dgate.astype(jnp.bfloat16), dup], axis=1)
    put(contract_last(inward, w_ref[:, 0 : 2 * UNITS]), 1)


VMEM = pl.BlockSpec(memory_space=pltpu.VMEM)
SMEM = pl.BlockSpec(memory_space=pltpu.SMEM)
HBM = pl.BlockSpec(memory_space=pltpu.HBM)


FIELD = jax.ShapeDtypeStruct((TOK, UNITS), jnp.float32)
W_SPACE = pltpu.VMEM((WIDTH, 3 * UNITS), jnp.bfloat16)
X_SPACE = pltpu.VMEM((TOK, WIDTH), jnp.bfloat16)
F_SPACE = pltpu.VMEM((TOK, UNITS), jnp.float32)


def early(strides, taps, bias, x_early, cot_t, w):
    return pl.pallas_call(
        early_kernel,
        out_shape=(jax.ShapeDtypeStruct((WIDTH, UNITS), jnp.bfloat16), FIELD, FIELD),
        in_specs=[SMEM, VMEM, VMEM, HBM, VMEM, HBM],
        out_specs=(VMEM, VMEM, VMEM),
        scratch_shapes=[
            W_SPACE,
            X_SPACE,
            pltpu.SemaphoreType.DMA((1, 8, 8)),
            pltpu.SemaphoreType.DMA((4,)),
        ],
        compiler_params=pltpu.CompilerParams(vmem_limit_bytes=36 * 1024 * 1024),
        cost_estimate=pl.CostEstimate(
            flops=3_000_000_000, transcendentals=0, bytes_accessed=8_000_000
        ),
        name="early",
    )(strides, taps, bias, x_early, cot_t, w)


def outputs(strides, taps, bias, x_late, cot, act, slope, w):
    piece = jax.ShapeDtypeStruct((NX, 2, 32, WIDTH), jnp.bfloat16)
    return pl.pallas_call(
        outputs_kernel,
        out_shape=(piece, piece),
        in_specs=[SMEM, VMEM, VMEM, HBM, HBM, HBM, HBM, HBM],
        out_specs=(VMEM, VMEM),
        scratch_shapes=[
            W_SPACE,
            X_SPACE,
            X_SPACE,
            F_SPACE,
            F_SPACE,
            pltpu.SemaphoreType.DMA((2, 8, 8)),
            pltpu.SemaphoreType.DMA((7,)),
        ],
        compiler_params=pltpu.CompilerParams(vmem_limit_bytes=36 * 1024 * 1024),
        cost_estimate=pl.CostEstimate(
            flops=4_000_000_000, transcendentals=0, bytes_accessed=12_000_000
        ),
        name="outputs",
    )(strides, taps, bias, x_late, cot, act, slope, w)


def assemble_kernel(place_ref, mine_ref, other_ref, y_ref, dx_ref, sems):
    x = place_ref[0]
    core = place_ref[1]
    copies = []
    for who, ref in enumerate((mine_ref, other_ref)):
        half = core if who == 0 else 1 - core
        for d in range(NX):
            at = pl.multiple_of(half * 128 + lax.rem(x + NX - d, NX) * 32, 32)
            for k, out in enumerate((y_ref, dx_ref)):
                copies.append(
                    pltpu.make_async_copy(
                        ref.at[d, k], out.at[pl.ds(at, 32)], sems.at[who, d, k]
                    )
                )
    for c in copies:
        c.start()
    for c in copies:
        c.wait()


def assemble(where, mine, other):
    out = jax.ShapeDtypeStruct((TOK, WIDTH), jnp.bfloat16)
    return pl.pallas_call(
        assemble_kernel,
        out_shape=(out, out),
        in_specs=[SMEM, VMEM, VMEM],
        out_specs=(HBM, HBM),
        scratch_shapes=[pltpu.SemaphoreType.DMA((2, NX, 2))],
        compiler_params=pltpu.CompilerParams(vmem_limit_bytes=4 * 1024 * 1024),
        name="assemble",
    )(where, mine, other)


def exchanged(value):
    return lax.ppermute(value, "c", [(0, 1), (1, 0)])


def moved(value, steps):
    return lax.ppermute(value, "x", [(i, (i + steps) % NX) for i in range(NX)])


def in_hbm(*values):
    return [pltpu.with_memory_space_constraint(v, pltpu.HBM) for v in values]


def f32_sum(pieces):
    return pieces.astype(jnp.float32).sum(axis=0).astype(jnp.bfloat16)


def shards(x_late, x_early, cotangent, w_gate, w_up, w_down, conv_taps, conv_bias, grad_down):
    core = lax.axis_index("c")
    x = lax.axis_index("x")
    offset = lax.axis_index(TP) * UNITS
    taps = lax.dynamic_slice_in_dim(conv_taps, offset, UNITS, 1)
    bias = lax.dynamic_slice_in_dim(conv_bias, offset, UNITS, 0)[None]
    mine = jnp.concatenate([w_gate, w_up, w_down.T], axis=1)
    near = lax.all_to_all(
        jnp.broadcast_to(mine[None], (8,) + mine.shape), AXES, 0, 0,
        tiled=True, axis_index_groups=FIRST,
    )
    w = lax.all_gather(near, AXES, axis_index_groups=SECOND)
    strides = jnp.stack([8 - 7 * core, 1 + 7 * core]).astype(jnp.int32)
    w, x_late, x_early = in_hbm(w, x_late, x_early)
    grad_part, act, slope = early(strides, taps, bias, x_early, cotangent.T, w)
    cot, act, slope = in_hbm(cotangent, act, slope)
    keep, give = outputs(strides, taps, bias, x_late, cot, act, slope, w)
    grad = lax.all_to_all(
        grad_part.reshape(8, 256, UNITS), AXES, 0, 0, tiled=True, axis_index_groups=SECOND
    )
    grad = f32_sum(grad).reshape(8, 32, UNITS)
    grad = lax.all_to_all(grad, AXES, 0, 0, tiled=True, axis_index_groups=FIRST)
    grad_down_out = grad_down + grad.astype(jnp.float32).sum(axis=0).T

    got = exchanged(give)

    def chip_piece(at):
        left = lax.dynamic_index_in_dim(keep, at, 0, keepdims=False)
        right = lax.dynamic_index_in_dim(got, at, 0, keepdims=False)
        return left.astype(jnp.float32) + right.astype(jnp.float32)

    total = chip_piece(x)
    for d in (2, 1, 3):
        sent = chip_piece(lax.rem(x + d, NX)).astype(jnp.bfloat16)
        arrived = moved(sent, d)
        total = total + arrived.astype(jnp.float32)
    total = total.astype(jnp.bfloat16)
    spread = {d: moved(total, d) for d in (2, 1, 3)}
    mine = jnp.stack([total] + [spread[d] for d in range(1, NX)])
    other = exchanged(mine)
    where = jnp.stack([x, core]).astype(jnp.int32)
    y_late, dx_early = assemble(where, mine, other)
    return (y_late, dx_early, grad_down_out)


def solution(mesh):
    torus = Mesh(mesh.devices.reshape(NZ, NY, NX, NC), AXES)
    return jax.shard_map(
        shards,
        mesh=torus,
        in_specs=(
            P(FS, None),
            P(FS, None),
            P(FS, None),
            P(FS, TP),
            P(FS, TP),
            P(TP, FS),
            P(),
            P(),
            P(TP, FS),
        ),
        out_specs=(P(FS, None), P(FS, None), P(TP, FS)),
        check_vma=False,
    )
```

```python
import jax
import jax.numpy as jnp
from jax import lax
from jax.experimental import pallas as pl
from jax.experimental.pallas import tpu as pltpu
from jax.sharding import Mesh
from jax.sharding import PartitionSpec as P

AXES = ("z", "y", "x", "c")
FS = ("z", "y")
TP = ("x", "c")
NZ, NY, NX, NC = 8, 8, 4, 2
UNITS = 512
TOK = 256
WIDTH = 2048


def place(z, y, x, c):
    return ((z * NY + y) * NX + x) * NC + c


def split_groups(core_along_y):
    groups = []
    for x in range(NX):
        for k in range(8):
            groups.append([place(k, y, x, core_along_y) for y in range(NY)])
            groups.append([place(z, k, x, 1 - core_along_y) for z in range(NZ)])
    return groups


FIRST = split_groups(0)
SECOND = split_groups(1)


def contract_last(left, right):
    return lax.dot_general(
        left, right, (((1,), (1,)), ((), ())), preferred_element_type=jnp.float32
    )


def shift_later(field, steps):
    row = lax.broadcasted_iota(jnp.int32, field.shape, 0)
    return jnp.where(row >= steps, pltpu.roll(field, steps, 0), 0.0)


def shift_earlier(field, steps):
    rows = field.shape[0]
    row = lax.broadcasted_iota(jnp.int32, field.shape, 0)
    return jnp.where(row < rows - steps, pltpu.roll(field, rows - steps, 0), 0.0)


def conv_and_up(both, taps_ref, bias_ref):
    t0, t1, t2 = taps_ref[0:1, :], taps_ref[1:2, :], taps_ref[2:3, :]
    gate = both[:, 0:UNITS].astype(jnp.bfloat16).astype(jnp.float32)
    up = both[:, UNITS : 2 * UNITS]
    conv = bias_ref[0:1, :] + t2 * gate + t1 * shift_later(gate, 1) + t0 * shift_later(gate, 2)
    return conv, up


def sigmoid(v):
    return 1.0 / (1.0 + jnp.exp(-v))


def block_copies(south, w_hbm, w_ref, w_sems, x_hbm, x_ref, x_sems):
    def w_copy(a, m, part):
        p = jnp.where(south, a, m)
        j = jnp.where(south, m, a)
        rows = pl.ds((a * 8 + m) * 32, 32)
        cols = pl.ds(0, 2 * UNITS) if part == 0 else pl.ds(2 * UNITS, UNITS)
        return pltpu.make_async_copy(
            w_hbm.at[p, j, :, cols], w_ref.at[rows, cols], w_sems.at[part, a, m]
        )

    def x_copy(k):
        cols = pl.ds(k * 512, 512)
        return pltpu.make_async_copy(x_hbm.at[:, cols], x_ref.at[:, cols], x_sems.at[k])

    return w_copy, x_copy


def start_inward(w_copy, x_copy):
    for k in range(4):
        x_copy(k).start()
        for a in (2 * k, 2 * k + 1):
            for m in range(8):
                w_copy(a, m, 0).start()


def gate_and_up(w_copy, x_copy, w_ref, x_ref):
    both = jnp.zeros((TOK, 2 * UNITS), jnp.float32)
    for k in range(4):
        x_copy(k).wait()
        for a in (2 * k, 2 * k + 1):
            for m in range(8):
                w_copy(a, m, 0).wait()
        both = both + jnp.dot(
            x_ref[:, k * 512 : (k + 1) * 512],
            w_ref[k * 512 : (k + 1) * 512, 0 : 2 * UNITS],
            preferred_element_type=jnp.float32,
        )
    return both


def early_kernel(
    stride_ref, taps_ref, bias_ref, xe_hbm, cot_t_ref, w_hbm,
    grad_hbm, act_hbm, slope_hbm,
    w_ref, xe_ref, grad_ref, act_ref, slope_ref, w_sems, x_sems, grad_sems, field_sems,
):
    outer = stride_ref[0]
    inner = stride_ref[1]
    w_copy, x_copy = block_copies(outer == 8, w_hbm, w_ref, w_sems, xe_hbm, xe_ref, x_sems)
    start_inward(w_copy, x_copy)
    both = gate_and_up(w_copy, x_copy, w_ref, xe_ref)
    conv, up = conv_and_up(both, taps_ref, bias_ref)
    sig = sigmoid(conv)
    act = conv * sig
    act_ref[...] = act
    slope_ref[...] = up * sig * (1.0 + conv * (1.0 - sig))
    sent = [
        pltpu.make_async_copy(act_ref, act_hbm, field_sems.at[0]),
        pltpu.make_async_copy(slope_ref, slope_hbm, field_sems.at[1]),
    ]
    for c in sent:
        c.start()
    hidden = (act * up).astype(jnp.bfloat16)
    for k in range(8):
        grad_ref[k * 256 : (k + 1) * 256, :] = jnp.dot(
            cot_t_ref[k * 256 : (k + 1) * 256, :], hidden, preferred_element_type=jnp.float32
        ).astype(jnp.bfloat16)
        for j in range(8):
            at = pl.multiple_of((k * outer + j * inner) * 32, 32)
            block = pltpu.make_async_copy(
                grad_ref.at[pl.ds((k * 8 + j) * 32, 32)],
                grad_hbm.at[pl.ds(at, 32)],
                grad_sems.at[k, j],
            )
            block.start()
            sent.append(block)
    for c in sent:
        c.wait()


def outputs_kernel(
    stride_ref, taps_ref, bias_ref, xl_hbm, cot_hbm, act_hbm, slope_hbm, w_hbm,
    keep_ref, give_ref, w_ref, xl_ref, cot_ref, act_ref, slope_ref, w_sems, x_sems,
):
    south = stride_ref[0] == 8
    w_copy, x_copy = block_copies(south, w_hbm, w_ref, w_sems, xl_hbm, xl_ref, x_sems)
    start_inward(w_copy, x_copy)
    rest = [
        pltpu.make_async_copy(cot_hbm, cot_ref, x_sems.at[4]),
        pltpu.make_async_copy(act_hbm, act_ref, x_sems.at[5]),
        pltpu.make_async_copy(slope_hbm, slope_ref, x_sems.at[6]),
    ] + [w_copy(a, m, 1) for a in range(8) for m in range(8)]
    for c in rest:
        c.start()

    def put(value, at):
        value = value.astype(jnp.bfloat16)

        @pl.when(south)
        def _():
            for k in range(NX):
                keep_ref[k, at] = value[k * 32 : (k + 1) * 32]
                give_ref[k, at] = value[128 + k * 32 : 128 + (k + 1) * 32]

        @pl.when(jnp.logical_not(south))
        def _():
            for k in range(NX):
                give_ref[k, at] = value[k * 32 : (k + 1) * 32]
                keep_ref[k, at] = value[128 + k * 32 : 128 + (k + 1) * 32]

    t0, t1, t2 = taps_ref[0:1, :], taps_ref[1:2, :], taps_ref[2:3, :]
    both = gate_and_up(w_copy, x_copy, w_ref, xl_ref)
    late, late_up = conv_and_up(both, taps_ref, bias_ref)
    late_hidden = (late * sigmoid(late) * late_up).astype(jnp.bfloat16)
    for c in rest:
        c.wait()
    w_down = w_ref[:, 2 * UNITS : 3 * UNITS]
    put(contract_last(late_hidden, w_down), 0)
    dhidden = jnp.dot(cot_ref[...], w_down, preferred_element_type=jnp.float32)
    dup = (dhidden * act_ref[...]).astype(jnp.bfloat16)
    dconv = dhidden * slope_ref[...]
    dgate = t2 * dconv + t1 * shift_earlier(dconv, 1) + t0 * shift_earlier(dconv, 2)
    inward = jnp.concatenate([dgate.astype(jnp.bfloat16), dup], axis=1)
    put(contract_last(inward, w_ref[:, 0 : 2 * UNITS]), 1)


VMEM = pl.BlockSpec(memory_space=pltpu.VMEM)
SMEM = pl.BlockSpec(memory_space=pltpu.SMEM)
HBM = pl.BlockSpec(memory_space=pltpu.HBM)


FIELD = jax.ShapeDtypeStruct((TOK, UNITS), jnp.float32)
W_SPACE = pltpu.VMEM((WIDTH, 3 * UNITS), jnp.bfloat16)
X_SPACE = pltpu.VMEM((TOK, WIDTH), jnp.bfloat16)
F_SPACE = pltpu.VMEM((TOK, UNITS), jnp.float32)


def early(strides, taps, bias, x_early, cot_t, w):
    return pl.pallas_call(
        early_kernel,
        out_shape=(jax.ShapeDtypeStruct((WIDTH, UNITS), jnp.bfloat16), FIELD, FIELD),
        in_specs=[SMEM, VMEM, VMEM, HBM, VMEM, HBM],
        out_specs=(HBM, HBM, HBM),
        scratch_shapes=[
            W_SPACE,
            X_SPACE,
            pltpu.VMEM((WIDTH, UNITS), jnp.bfloat16),
            F_SPACE,
            F_SPACE,
            pltpu.SemaphoreType.DMA((1, 8, 8)),
            pltpu.SemaphoreType.DMA((4,)),
            pltpu.SemaphoreType.DMA((8, 8)),
            pltpu.SemaphoreType.DMA((2,)),
        ],
        compiler_params=pltpu.CompilerParams(vmem_limit_bytes=36 * 1024 * 1024),
        cost_estimate=pl.CostEstimate(
            flops=3_000_000_000, transcendentals=0, bytes_accessed=8_000_000
        ),
        name="early",
    )(strides, taps, bias, x_early, cot_t, w)


def outputs(strides, taps, bias, x_late, cot, act, slope, w):
    piece = jax.ShapeDtypeStruct((NX, 2, 32, WIDTH), jnp.bfloat16)
    return pl.pallas_call(
        outputs_kernel,
        out_shape=(piece, piece),
        in_specs=[SMEM, VMEM, VMEM, HBM, HBM, HBM, HBM, HBM],
        out_specs=(VMEM, VMEM),
        scratch_shapes=[
            W_SPACE,
            X_SPACE,
            X_SPACE,
            F_SPACE,
            F_SPACE,
            pltpu.SemaphoreType.DMA((2, 8, 8)),
            pltpu.SemaphoreType.DMA((7,)),
        ],
        compiler_params=pltpu.CompilerParams(vmem_limit_bytes=36 * 1024 * 1024),
        cost_estimate=pl.CostEstimate(
            flops=4_000_000_000, transcendentals=0, bytes_accessed=12_000_000
        ),
        name="outputs",
    )(strides, taps, bias, x_late, cot, act, slope, w)


def assemble_kernel(place_ref, mine_ref, other_ref, y_ref, dx_ref, sems):
    x = place_ref[0]
    core = place_ref[1]
    copies = []
    for who, ref in enumerate((mine_ref, other_ref)):
        half = core if who == 0 else 1 - core
        for d in range(NX):
            at = pl.multiple_of(half * 128 + lax.rem(x + NX - d, NX) * 32, 32)
            for k, out in enumerate((y_ref, dx_ref)):
                copies.append(
                    pltpu.make_async_copy(
                        ref.at[d, k], out.at[pl.ds(at, 32)], sems.at[who, d, k]
                    )
                )
    for c in copies:
        c.start()
    for c in copies:
        c.wait()


def assemble(where, mine, other):
    out = jax.ShapeDtypeStruct((TOK, WIDTH), jnp.bfloat16)
    return pl.pallas_call(
        assemble_kernel,
        out_shape=(out, out),
        in_specs=[SMEM, VMEM, VMEM],
        out_specs=(HBM, HBM),
        scratch_shapes=[pltpu.SemaphoreType.DMA((2, NX, 2))],
        compiler_params=pltpu.CompilerParams(vmem_limit_bytes=4 * 1024 * 1024),
        name="assemble",
    )(where, mine, other)


def exchanged(value):
    return lax.ppermute(value, "c", [(0, 1), (1, 0)])


def moved(value, steps):
    return lax.ppermute(value, "x", [(i, (i + steps) % NX) for i in range(NX)])


def in_hbm(*values):
    return [pltpu.with_memory_space_constraint(v, pltpu.HBM) for v in values]


def f32_sum(pieces):
    return pieces.astype(jnp.float32).sum(axis=0).astype(jnp.bfloat16)


def shards(x_late, x_early, cotangent, w_gate, w_up, w_down, conv_taps, conv_bias, grad_down):
    core = lax.axis_index("c")
    x = lax.axis_index("x")
    offset = lax.axis_index(TP) * UNITS
    taps = lax.dynamic_slice_in_dim(conv_taps, offset, UNITS, 1)
    bias = lax.dynamic_slice_in_dim(conv_bias, offset, UNITS, 0)[None]
    mine = jnp.concatenate([w_gate, w_up, w_down.T], axis=1)
    near = lax.all_to_all(
        jnp.broadcast_to(mine[None], (8,) + mine.shape), AXES, 0, 0,
        tiled=True, axis_index_groups=FIRST,
    )
    w = lax.all_gather(near, AXES, axis_index_groups=SECOND)
    strides = jnp.stack([8 - 7 * core, 1 + 7 * core]).astype(jnp.int32)
    w, x_late, x_early = in_hbm(w, x_late, x_early)
    grad_part, act, slope = early(strides, taps, bias, x_early, cotangent.T, w)
    cot, act, slope = in_hbm(cotangent, act, slope)
    keep, give = outputs(strides, taps, bias, x_late, cot, act, slope, w)
    grad = lax.all_to_all(
        grad_part.reshape(8, 256, UNITS), AXES, 0, 0, tiled=True, axis_index_groups=SECOND
    )
    grad = f32_sum(grad).reshape(8, 32, UNITS)
    grad = lax.all_to_all(grad, AXES, 0, 0, tiled=True, axis_index_groups=FIRST)
    grad_down_out = grad_down + grad.astype(jnp.float32).sum(axis=0).T

    got = exchanged(give)

    def chip_piece(at):
        left = lax.dynamic_index_in_dim(keep, at, 0, keepdims=False)
        right = lax.dynamic_index_in_dim(got, at, 0, keepdims=False)
        return left.astype(jnp.float32) + right.astype(jnp.float32)

    total = chip_piece(x)
    for d in (2, 1, 3):
        sent = chip_piece(lax.rem(x + d, NX)).astype(jnp.bfloat16)
        arrived = moved(sent, d)
        total = total + arrived.astype(jnp.float32)
    total = total.astype(jnp.bfloat16)
    spread = {d: moved(total, d) for d in (2, 1, 3)}
    mine = jnp.stack([total] + [spread[d] for d in range(1, NX)])
    other = exchanged(mine)
    where = jnp.stack([x, core]).astype(jnp.int32)
    y_late, dx_early = assemble(where, mine, other)
    return (y_late, dx_early, grad_down_out)


def solution(mesh):
    torus = Mesh(mesh.devices.reshape(NZ, NY, NX, NC), AXES)
    return jax.shard_map(
        shards,
        mesh=torus,
        in_specs=(
            P(FS, None),
            P(FS, None),
            P(FS, None),
            P(FS, TP),
            P(FS, TP),
            P(TP, FS),
            P(),
            P(),
            P(TP, FS),
        ),
        out_specs=(P(FS, None), P(FS, None), P(TP, FS)),
        check_vma=False,
    )
```

```python
import jax
import jax.numpy as jnp
from jax import lax
from jax.experimental import pallas as pl
from jax.experimental.pallas import tpu as pltpu
from jax.sharding import Mesh
from jax.sharding import PartitionSpec as P

AXES = ("z", "y", "x", "c")
FS = ("z", "y")
TP = ("x", "c")
NZ, NY, NX, NC = 8, 8, 4, 2
UNITS = 512
TOK = 256
WIDTH = 2048


def place(z, y, x, c):
    return ((z * NY + y) * NX + x) * NC + c


def split_groups(core_along_y):
    groups = []
    for x in range(NX):
        for k in range(8):
            groups.append([place(k, y, x, core_along_y) for y in range(NY)])
            groups.append([place(z, k, x, 1 - core_along_y) for z in range(NZ)])
    return groups


FIRST = split_groups(0)
SECOND = split_groups(1)


def contract_last(left, right):
    return lax.dot_general(
        left, right, (((1,), (1,)), ((), ())), preferred_element_type=jnp.float32
    )


def shift_later(field, steps):
    row = lax.broadcasted_iota(jnp.int32, field.shape, 0)
    return jnp.where(row >= steps, pltpu.roll(field, steps, 0), 0.0)


def shift_earlier(field, steps):
    rows = field.shape[0]
    row = lax.broadcasted_iota(jnp.int32, field.shape, 0)
    return jnp.where(row < rows - steps, pltpu.roll(field, rows - steps, 0), 0.0)


def conv_and_up(both, taps_ref, bias_ref):
    t0, t1, t2 = taps_ref[0:1, :], taps_ref[1:2, :], taps_ref[2:3, :]
    gate = both[:, 0:UNITS].astype(jnp.bfloat16).astype(jnp.float32)
    up = both[:, UNITS : 2 * UNITS]
    conv = bias_ref[0:1, :] + t2 * gate + t1 * shift_later(gate, 1) + t0 * shift_later(gate, 2)
    return conv, up


def sigmoid(v):
    return 1.0 / (1.0 + jnp.exp(-v))


def block_copies(south, w_hbm, w_ref, w_sems, x_hbm, x_ref, x_sems):
    def w_copy(a, m, part):
        p = jnp.where(south, a, m)
        j = jnp.where(south, m, a)
        rows = pl.ds((a * 8 + m) * 32, 32)
        cols = pl.ds(0, 2 * UNITS) if part == 0 else pl.ds(2 * UNITS, UNITS)
        return pltpu.make_async_copy(
            w_hbm.at[p, j, :, cols], w_ref.at[rows, cols], w_sems.at[part, a, m]
        )

    def x_copy(k):
        cols = pl.ds(k * 512, 512)
        return pltpu.make_async_copy(x_hbm.at[:, cols], x_ref.at[:, cols], x_sems.at[k])

    return w_copy, x_copy


def start_inward(w_copy, x_copy):
    for k in range(4):
        x_copy(k).start()
        for a in (2 * k, 2 * k + 1):
            for m in range(8):
                w_copy(a, m, 0).start()


def gate_and_up(w_copy, x_copy, w_ref, x_ref):
    both = jnp.zeros((TOK, 2 * UNITS), jnp.float32)
    for k in range(4):
        x_copy(k).wait()
        for a in (2 * k, 2 * k + 1):
            for m in range(8):
                w_copy(a, m, 0).wait()
        both = both + jnp.dot(
            x_ref[:, k * 512 : (k + 1) * 512],
            w_ref[k * 512 : (k + 1) * 512, 0 : 2 * UNITS],
            preferred_element_type=jnp.float32,
        )
    return both


def early_kernel(
    stride_ref, taps_ref, bias_ref, xe_hbm, cot_t_hbm, w_hbm,
    grad_hbm, act_hbm, slope_hbm,
    w_ref, xe_ref, cot_t_ref, grad_ref, act_ref, slope_ref, w_sems, x_sems, grad_sems, field_sems,
):
    outer = stride_ref[0]
    inner = stride_ref[1]
    w_copy, x_copy = block_copies(outer == 8, w_hbm, w_ref, w_sems, xe_hbm, xe_ref, x_sems)
    start_inward(w_copy, x_copy)
    cot_copy = pltpu.make_async_copy(cot_t_hbm, cot_t_ref, field_sems.at[2])
    cot_copy.start()
    both = gate_and_up(w_copy, x_copy, w_ref, xe_ref)
    conv, up = conv_and_up(both, taps_ref, bias_ref)
    sig = sigmoid(conv)
    act = conv * sig
    act_ref[...] = act
    slope_ref[...] = up * sig * (1.0 + conv * (1.0 - sig))
    sent = [
        pltpu.make_async_copy(act_ref, act_hbm, field_sems.at[0]),
        pltpu.make_async_copy(slope_ref, slope_hbm, field_sems.at[1]),
    ]
    for c in sent:
        c.start()
    hidden = (act * up).astype(jnp.bfloat16)
    cot_copy.wait()
    for k in range(8):
        grad_ref[k * 256 : (k + 1) * 256, :] = jnp.dot(
            cot_t_ref[k * 256 : (k + 1) * 256, :], hidden, preferred_element_type=jnp.float32
        ).astype(jnp.bfloat16)
        for j in range(8):
            at = pl.multiple_of((k * outer + j * inner) * 32, 32)
            block = pltpu.make_async_copy(
                grad_ref.at[pl.ds((k * 8 + j) * 32, 32)],
                grad_hbm.at[pl.ds(at, 32)],
                grad_sems.at[k, j],
            )
            block.start()
            sent.append(block)
    for c in sent:
        c.wait()


def outputs_kernel(
    stride_ref, taps_ref, bias_ref, xl_hbm, cot_hbm, act_hbm, slope_hbm, w_hbm,
    keep_ref, give_ref, w_ref, xl_ref, cot_ref, act_ref, slope_ref, w_sems, x_sems,
):
    south = stride_ref[0] == 8
    w_copy, x_copy = block_copies(south, w_hbm, w_ref, w_sems, xl_hbm, xl_ref, x_sems)
    start_inward(w_copy, x_copy)
    rest = [
        pltpu.make_async_copy(cot_hbm, cot_ref, x_sems.at[4]),
        pltpu.make_async_copy(act_hbm, act_ref, x_sems.at[5]),
        pltpu.make_async_copy(slope_hbm, slope_ref, x_sems.at[6]),
    ] + [w_copy(a, m, 1) for a in range(8) for m in range(8)]
    for c in rest:
        c.start()

    def put(value, at):
        value = value.astype(jnp.bfloat16)

        @pl.when(south)
        def _():
            for k in range(NX):
                keep_ref[k, at] = value[k * 32 : (k + 1) * 32]
                give_ref[k, at] = value[128 + k * 32 : 128 + (k + 1) * 32]

        @pl.when(jnp.logical_not(south))
        def _():
            for k in range(NX):
                give_ref[k, at] = value[k * 32 : (k + 1) * 32]
                keep_ref[k, at] = value[128 + k * 32 : 128 + (k + 1) * 32]

    t0, t1, t2 = taps_ref[0:1, :], taps_ref[1:2, :], taps_ref[2:3, :]
    both = gate_and_up(w_copy, x_copy, w_ref, xl_ref)
    late, late_up = conv_and_up(both, taps_ref, bias_ref)
    late_hidden = (late * sigmoid(late) * late_up).astype(jnp.bfloat16)
    for c in rest:
        c.wait()
    w_down = w_ref[:, 2 * UNITS : 3 * UNITS]
    put(contract_last(late_hidden, w_down), 0)
    dhidden = jnp.dot(cot_ref[...], w_down, preferred_element_type=jnp.float32)
    dup = (dhidden * act_ref[...]).astype(jnp.bfloat16)
    dconv = dhidden * slope_ref[...]
    dgate = t2 * dconv + t1 * shift_earlier(dconv, 1) + t0 * shift_earlier(dconv, 2)
    inward = jnp.concatenate([dgate.astype(jnp.bfloat16), dup], axis=1)
    put(contract_last(inward, w_ref[:, 0 : 2 * UNITS]), 1)


VMEM = pl.BlockSpec(memory_space=pltpu.VMEM)
SMEM = pl.BlockSpec(memory_space=pltpu.SMEM)
HBM = pl.BlockSpec(memory_space=pltpu.HBM)


FIELD = jax.ShapeDtypeStruct((TOK, UNITS), jnp.float32)
W_SPACE = pltpu.VMEM((WIDTH, 3 * UNITS), jnp.bfloat16)
X_SPACE = pltpu.VMEM((TOK, WIDTH), jnp.bfloat16)
F_SPACE = pltpu.VMEM((TOK, UNITS), jnp.float32)


def early(strides, taps, bias, x_early, cot_t, w):
    return pl.pallas_call(
        early_kernel,
        out_shape=(jax.ShapeDtypeStruct((WIDTH, UNITS), jnp.bfloat16), FIELD, FIELD),
        in_specs=[SMEM, VMEM, VMEM, HBM, HBM, HBM],
        out_specs=(HBM, HBM, HBM),
        scratch_shapes=[
            W_SPACE,
            X_SPACE,
            pltpu.VMEM((WIDTH, TOK), jnp.bfloat16),
            pltpu.VMEM((WIDTH, UNITS), jnp.bfloat16),
            F_SPACE,
            F_SPACE,
            pltpu.SemaphoreType.DMA((1, 8, 8)),
            pltpu.SemaphoreType.DMA((4,)),
            pltpu.SemaphoreType.DMA((8, 8)),
            pltpu.SemaphoreType.DMA((3,)),
        ],
        compiler_params=pltpu.CompilerParams(vmem_limit_bytes=58 * 1024 * 1024),
        cost_estimate=pl.CostEstimate(
            flops=3_000_000_000, transcendentals=0, bytes_accessed=8_000_000
        ),
        name="early",
    )(strides, taps, bias, x_early, cot_t, w)


def outputs(strides, taps, bias, x_late, cot, act, slope, w):
    piece = jax.ShapeDtypeStruct((NX, 2, 32, WIDTH), jnp.bfloat16)
    return pl.pallas_call(
        outputs_kernel,
        out_shape=(piece, piece),
        in_specs=[SMEM, VMEM, VMEM, HBM, HBM, HBM, HBM, HBM],
        out_specs=(VMEM, VMEM),
        scratch_shapes=[
            W_SPACE,
            X_SPACE,
            X_SPACE,
            F_SPACE,
            F_SPACE,
            pltpu.SemaphoreType.DMA((2, 8, 8)),
            pltpu.SemaphoreType.DMA((7,)),
        ],
        compiler_params=pltpu.CompilerParams(vmem_limit_bytes=36 * 1024 * 1024),
        cost_estimate=pl.CostEstimate(
            flops=4_000_000_000, transcendentals=0, bytes_accessed=12_000_000
        ),
        name="outputs",
    )(strides, taps, bias, x_late, cot, act, slope, w)


def assemble_kernel(place_ref, mine_ref, other_ref, y_ref, dx_ref, sems):
    x = place_ref[0]
    core = place_ref[1]
    copies = []
    for who, ref in enumerate((mine_ref, other_ref)):
        half = core if who == 0 else 1 - core
        for d in range(NX):
            at = pl.multiple_of(half * 128 + lax.rem(x + NX - d, NX) * 32, 32)
            for k, out in enumerate((y_ref, dx_ref)):
                copies.append(
                    pltpu.make_async_copy(
                        ref.at[d, k], out.at[pl.ds(at, 32)], sems.at[who, d, k]
                    )
                )
    for c in copies:
        c.start()
    for c in copies:
        c.wait()


def assemble(where, mine, other):
    out = jax.ShapeDtypeStruct((TOK, WIDTH), jnp.bfloat16)
    return pl.pallas_call(
        assemble_kernel,
        out_shape=(out, out),
        in_specs=[SMEM, VMEM, VMEM],
        out_specs=(HBM, HBM),
        scratch_shapes=[pltpu.SemaphoreType.DMA((2, NX, 2))],
        compiler_params=pltpu.CompilerParams(vmem_limit_bytes=4 * 1024 * 1024),
        name="assemble",
    )(where, mine, other)


def exchanged(value):
    return lax.ppermute(value, "c", [(0, 1), (1, 0)])


def moved(value, steps):
    return lax.ppermute(value, "x", [(i, (i + steps) % NX) for i in range(NX)])


def in_hbm(*values):
    return [pltpu.with_memory_space_constraint(v, pltpu.HBM) for v in values]


def f32_sum(pieces):
    return pieces.astype(jnp.float32).sum(axis=0).astype(jnp.bfloat16)


def shards(x_late, x_early, cotangent, w_gate, w_up, w_down, conv_taps, conv_bias, grad_down):
    core = lax.axis_index("c")
    x = lax.axis_index("x")
    offset = lax.axis_index(TP) * UNITS
    taps = lax.dynamic_slice_in_dim(conv_taps, offset, UNITS, 1)
    bias = lax.dynamic_slice_in_dim(conv_bias, offset, UNITS, 0)[None]
    mine = jnp.concatenate([w_gate, w_up, w_down.T], axis=1)
    near = lax.all_to_all(
        jnp.broadcast_to(mine[None], (8,) + mine.shape), AXES, 0, 0,
        tiled=True, axis_index_groups=FIRST,
    )
    w = lax.all_gather(near, AXES, axis_index_groups=SECOND)
    strides = jnp.stack([8 - 7 * core, 1 + 7 * core]).astype(jnp.int32)
    w, x_late, x_early = in_hbm(w, x_late, x_early)
    grad_part, act, slope = early(strides, taps, bias, x_early, cotangent.T, w)
    cot, act, slope = in_hbm(cotangent, act, slope)
    keep, give = outputs(strides, taps, bias, x_late, cot, act, slope, w)
    grad = lax.all_to_all(
        grad_part.reshape(8, 256, UNITS), AXES, 0, 0, tiled=True, axis_index_groups=SECOND
    )
    grad = f32_sum(grad).reshape(8, 32, UNITS)
    grad = lax.all_to_all(grad, AXES, 0, 0, tiled=True, axis_index_groups=FIRST)
    grad_down_out = grad_down + grad.astype(jnp.float32).sum(axis=0).T

    got = exchanged(give)

    def chip_piece(at):
        left = lax.dynamic_index_in_dim(keep, at, 0, keepdims=False)
        right = lax.dynamic_index_in_dim(got, at, 0, keepdims=False)
        return left.astype(jnp.float32) + right.astype(jnp.float32)

    total = chip_piece(x)
    for d in range(1, NX):
        sent = chip_piece(lax.rem(x + d, NX)).astype(jnp.bfloat16)
        arrived = moved(sent, d)
        total = total + arrived.astype(jnp.float32)
    total = total.astype(jnp.bfloat16)
    spread = {d: moved(total, d) for d in range(1, NX)}
    mine = jnp.stack([total] + [spread[d] for d in range(1, NX)])
    other = exchanged(mine)
    where = jnp.stack([x, core]).astype(jnp.int32)
    y_late, dx_early = assemble(where, mine, other)
    return (y_late, dx_early, grad_down_out)


def solution(mesh):
    torus = Mesh(mesh.devices.reshape(NZ, NY, NX, NC), AXES)
    return jax.shard_map(
        shards,
        mesh=torus,
        in_specs=(
            P(FS, None),
            P(FS, None),
            P(FS, None),
            P(FS, TP),
            P(FS, TP),
            P(TP, FS),
            P(),
            P(),
            P(TP, FS),
        ),
        out_specs=(P(FS, None), P(FS, None), P(TP, FS)),
        check_vma=False,
    )
```

```python
import jax
import jax.numpy as jnp
from jax import lax
from jax.experimental import pallas as pl
from jax.experimental.pallas import tpu as pltpu
from jax.sharding import Mesh
from jax.sharding import PartitionSpec as P

AXES = ("z", "y", "x", "c")
FS = ("z", "y")
TP = ("x", "c")
NZ, NY, NX, NC = 8, 8, 4, 2
UNITS = 512
TOK = 256
WIDTH = 2048


def place(z, y, x, c):
    return ((z * NY + y) * NX + x) * NC + c


def split_groups(core_along_y):
    groups = []
    for x in range(NX):
        for k in range(8):
            groups.append([place(k, y, x, core_along_y) for y in range(NY)])
            groups.append([place(z, k, x, 1 - core_along_y) for z in range(NZ)])
    return groups


FIRST = split_groups(0)
SECOND = split_groups(1)


def contract_last(left, right):
    return lax.dot_general(
        left, right, (((1,), (1,)), ((), ())), preferred_element_type=jnp.float32
    )


def shift_later(field, steps):
    row = lax.broadcasted_iota(jnp.int32, field.shape, 0)
    return jnp.where(row >= steps, pltpu.roll(field, steps, 0), 0.0)


def shift_earlier(field, steps):
    rows = field.shape[0]
    row = lax.broadcasted_iota(jnp.int32, field.shape, 0)
    return jnp.where(row < rows - steps, pltpu.roll(field, rows - steps, 0), 0.0)


def conv_and_up(both, taps_ref, bias_ref):
    t0, t1, t2 = taps_ref[0:1, :], taps_ref[1:2, :], taps_ref[2:3, :]
    gate = both[:, 0:UNITS].astype(jnp.bfloat16).astype(jnp.float32)
    up = both[:, UNITS : 2 * UNITS]
    conv = bias_ref[0:1, :] + t2 * gate + t1 * shift_later(gate, 1) + t0 * shift_later(gate, 2)
    return conv, up


def sigmoid(v):
    return 1.0 / (1.0 + jnp.exp(-v))


def layer_kernel(
    stride_ref, taps_ref, bias_ref, xe_hbm, xl_hbm, cot_ref, w_hbm,
    keep_ref, give_ref, hidden_ref, w_ref, xe_ref, xl_ref, w_sems, x_sems,
):
    south = stride_ref[0] == 8

    def w_copy(a, m, part):
        p = jnp.where(south, a, m)
        j = jnp.where(south, m, a)
        rows = pl.ds((a * 8 + m) * 32, 32)
        cols = pl.ds(0, 2 * UNITS) if part == 0 else pl.ds(2 * UNITS, UNITS)
        return pltpu.make_async_copy(
            w_hbm.at[p, j, :, cols], w_ref.at[rows, cols], w_sems.at[part, a, m]
        )

    blocks = [(a, m) for a in range(8) for m in range(8)]
    xl_copy = pltpu.make_async_copy(xl_hbm, xl_ref, x_sems.at[4])

    def xe_copy(k):
        cols = pl.ds(k * 512, 512)
        return pltpu.make_async_copy(xe_hbm.at[:, cols], xe_ref.at[:, cols], x_sems.at[k])

    for a, m in blocks:
        if a % 2 == 0 and m == 0:
            xe_copy(a // 2).start()
        w_copy(a, m, 0).start()
    xl_copy.start()
    for a, m in blocks:
        w_copy(a, m, 1).start()

    def put(value, at):
        value = value.astype(jnp.bfloat16)

        @pl.when(south)
        def _():
            for k in range(NX):
                keep_ref[k, at] = value[k * 32 : (k + 1) * 32]
                give_ref[k, at] = value[128 + k * 32 : 128 + (k + 1) * 32]

        @pl.when(jnp.logical_not(south))
        def _():
            for k in range(NX):
                give_ref[k, at] = value[k * 32 : (k + 1) * 32]
                keep_ref[k, at] = value[128 + k * 32 : 128 + (k + 1) * 32]

    t0, t1, t2 = taps_ref[0:1, :], taps_ref[1:2, :], taps_ref[2:3, :]
    both = jnp.zeros((TOK, 2 * UNITS), jnp.float32)
    for k in range(4):
        xe_copy(k).wait()
        for a in (2 * k, 2 * k + 1):
            for m in range(8):
                w_copy(a, m, 0).wait()
        both = both + jnp.dot(
            xe_ref[:, k * 512 : (k + 1) * 512],
            w_ref[k * 512 : (k + 1) * 512, 0 : 2 * UNITS],
            preferred_element_type=jnp.float32,
        )
    conv, up = conv_and_up(both, taps_ref, bias_ref)
    sig = sigmoid(conv)
    act = conv * sig
    hidden_ref[...] = (act * up).astype(jnp.bfloat16)
    slope = up * sig * (1.0 + conv * (1.0 - sig))
    xl_copy.wait()
    late, late_up = conv_and_up(
        jnp.dot(xl_ref[...], w_ref[:, 0 : 2 * UNITS], preferred_element_type=jnp.float32),
        taps_ref,
        bias_ref,
    )
    late_hidden = (late * sigmoid(late) * late_up).astype(jnp.bfloat16)
    for a, m in blocks:
        w_copy(a, m, 1).wait()
    w_down = w_ref[:, 2 * UNITS : 3 * UNITS]
    dhidden = jnp.dot(cot_ref[...], w_down, preferred_element_type=jnp.float32)
    dup = (dhidden * act).astype(jnp.bfloat16)
    dconv = dhidden * slope
    dgate = t2 * dconv + t1 * shift_earlier(dconv, 1) + t0 * shift_earlier(dconv, 2)
    inward = jnp.concatenate([dgate.astype(jnp.bfloat16), dup], axis=1)
    put(contract_last(inward, w_ref[:, 0 : 2 * UNITS]), 1)
    put(contract_last(late_hidden, w_down), 0)


VMEM = pl.BlockSpec(memory_space=pltpu.VMEM)
SMEM = pl.BlockSpec(memory_space=pltpu.SMEM)
HBM = pl.BlockSpec(memory_space=pltpu.HBM)


def layer(strides, taps, bias, x_early, x_late, cot, w):
    piece = jax.ShapeDtypeStruct((NX, 2, 32, WIDTH), jnp.bfloat16)
    return pl.pallas_call(
        layer_kernel,
        out_shape=(piece, piece, jax.ShapeDtypeStruct((TOK, UNITS), jnp.bfloat16)),
        in_specs=[SMEM, VMEM, VMEM, HBM, HBM, VMEM, HBM],
        out_specs=(VMEM, VMEM, VMEM),
        scratch_shapes=[
            pltpu.VMEM((WIDTH, 3 * UNITS), jnp.bfloat16),
            pltpu.VMEM((TOK, WIDTH), jnp.bfloat16),
            pltpu.VMEM((TOK, WIDTH), jnp.bfloat16),
            pltpu.SemaphoreType.DMA((2, 8, 8)),
            pltpu.SemaphoreType.DMA((5,)),
        ],
        compiler_params=pltpu.CompilerParams(vmem_limit_bytes=36 * 1024 * 1024),
        cost_estimate=pl.CostEstimate(
            flops=6_000_000_000, transcendentals=0, bytes_accessed=12_000_000
        ),
        name="layer",
    )(strides, taps, bias, x_early, x_late, cot, w)


def gradient_kernel(stride_ref, cot_t_ref, hidden_ref, grad_ref):
    outer = stride_ref[0]
    inner = stride_ref[1]
    for k in range(8):
        part = jnp.dot(
            cot_t_ref[k * 256 : (k + 1) * 256, :],
            hidden_ref[...],
            preferred_element_type=jnp.float32,
        ).astype(jnp.bfloat16)
        for j in range(8):
            at = pl.multiple_of((k * outer + j * inner) * 32, 32)
            grad_ref[pl.ds(at, 32), :] = part[j * 32 : (j + 1) * 32, :]


def gradient(strides, cot_t, hidden):
    return pl.pallas_call(
        gradient_kernel,
        out_shape=jax.ShapeDtypeStruct((WIDTH, UNITS), jnp.bfloat16),
        in_specs=[SMEM, VMEM, VMEM],
        out_specs=VMEM,
        compiler_params=pltpu.CompilerParams(vmem_limit_bytes=16 * 1024 * 1024),
        cost_estimate=pl.CostEstimate(
            flops=1_000_000_000, transcendentals=0, bytes_accessed=4_000_000
        ),
        name="gradient",
    )(strides, cot_t, hidden)


def assemble_kernel(place_ref, mine_ref, other_ref, y_ref, dx_ref, sems):
    x = place_ref[0]
    core = place_ref[1]
    copies = []
    for who, ref in enumerate((mine_ref, other_ref)):
        half = core if who == 0 else 1 - core
        for d in range(NX):
            at = pl.multiple_of(half * 128 + lax.rem(x + NX - d, NX) * 32, 32)
            for k, out in enumerate((y_ref, dx_ref)):
                copies.append(
                    pltpu.make_async_copy(
                        ref.at[d, k], out.at[pl.ds(at, 32)], sems.at[who, d, k]
                    )
                )
    for c in copies:
        c.start()
    for c in copies:
        c.wait()


def assemble(where, mine, other):
    out = jax.ShapeDtypeStruct((TOK, WIDTH), jnp.bfloat16)
    return pl.pallas_call(
        assemble_kernel,
        out_shape=(out, out),
        in_specs=[SMEM, VMEM, VMEM],
        out_specs=(HBM, HBM),
        scratch_shapes=[pltpu.SemaphoreType.DMA((2, NX, 2))],
        compiler_params=pltpu.CompilerParams(vmem_limit_bytes=4 * 1024 * 1024),
        name="assemble",
    )(where, mine, other)


def exchanged(value):
    return lax.ppermute(value, "c", [(0, 1), (1, 0)])


def moved(value, steps):
    return lax.ppermute(value, "x", [(i, (i + steps) % NX) for i in range(NX)])


def f32_sum(pieces):
    return pieces.astype(jnp.float32).sum(axis=0).astype(jnp.bfloat16)


def shards(x_late, x_early, cotangent, w_gate, w_up, w_down, conv_taps, conv_bias, grad_down):
    core = lax.axis_index("c")
    x = lax.axis_index("x")
    offset = lax.axis_index(TP) * UNITS
    taps = lax.dynamic_slice_in_dim(conv_taps, offset, UNITS, 1)
    bias = lax.dynamic_slice_in_dim(conv_bias, offset, UNITS, 0)[None]
    mine = jnp.concatenate([w_gate, w_up, w_down.T], axis=1)
    near = lax.all_to_all(
        jnp.broadcast_to(mine[None], (8,) + mine.shape), AXES, 0, 0,
        tiled=True, axis_index_groups=FIRST,
    )
    w = lax.all_gather(near, AXES, axis_index_groups=SECOND)
    w, x_late, x_early = (
        pltpu.with_memory_space_constraint(v, pltpu.HBM) for v in (w, x_late, x_early)
    )
    strides = jnp.stack([8 - 7 * core, 1 + 7 * core]).astype(jnp.int32)
    keep, give, hidden = layer(strides, taps, bias, x_early, x_late, cotangent, w)
    grad_part = gradient(strides, cotangent.T, hidden)
    grad = lax.all_to_all(
        grad_part.reshape(8, 256, UNITS), AXES, 0, 0, tiled=True, axis_index_groups=SECOND
    )
    grad = f32_sum(grad).reshape(8, 32, UNITS)
    grad = lax.all_to_all(grad, AXES, 0, 0, tiled=True, axis_index_groups=FIRST)
    grad_down_out = grad_down + grad.astype(jnp.float32).sum(axis=0).T

    got = exchanged(give)

    def chip_piece(at):
        left = lax.dynamic_index_in_dim(keep, at, 0, keepdims=False)
        right = lax.dynamic_index_in_dim(got, at, 0, keepdims=False)
        return left.astype(jnp.float32) + right.astype(jnp.float32)

    total = chip_piece(x)
    for d in range(1, NX):
        sent = chip_piece(lax.rem(x + d, NX)).astype(jnp.bfloat16)
        arrived = moved(sent, d)
        total = total + arrived.astype(jnp.float32)
    total = total.astype(jnp.bfloat16)
    spread = [moved(total, d) for d in range(1, NX)]
    mine = jnp.stack([total] + spread)
    other = exchanged(mine)
    where = jnp.stack([x, core]).astype(jnp.int32)
    y_late, dx_early = assemble(where, mine, other)
    return (y_late, dx_early, grad_down_out)


def solution(mesh):
    torus = Mesh(mesh.devices.reshape(NZ, NY, NX, NC), AXES)
    return jax.shard_map(
        shards,
        mesh=torus,
        in_specs=(
            P(FS, None),
            P(FS, None),
            P(FS, None),
            P(FS, TP),
            P(FS, TP),
            P(TP, FS),
            P(),
            P(),
            P(TP, FS),
        ),
        out_specs=(P(FS, None), P(FS, None), P(TP, FS)),
        check_vma=False,
    )
```
